512 devices in a mesh: sp: 32 (over z, x), tp: 16 (over y, core).
Axes of the slice: x: 4, y: 8, z: 8, core: 2. Of those that a mesh axis runs over, the one named last changes fastest.
Arguments:
- conv_value: bfloat16 [8192, 1024], P('sp', 'tp'), may hold values from -15 to 15
- conv_gate: bfloat16 [8192, 1024], P('sp', 'tp'), may hold values from -8 to 8
- conv_taps: bfloat16 [31, 1024], P(None, 'tp'), may hold values from -1 to 1
- conv_gain: float32 [1024], P('tp'), may hold values from 0.1 to 1.9
- out_weight: bfloat16 [1024, 2048], P('tp'), may hold values from -0.1875 to 0.1875
- residual: bfloat16 [8192, 2048], P('sp'), may hold values from -6 to 6
- route_ids: int32 [8192, 2], P('sp'), may hold values from 0 to 31, all different within a row; in each aligned block of 256 rows (0 to 255, 256 to 511, ...) at most 32 rows name the same one
- route_weight: float32 [8192, 2], P('sp'), may hold values from 0.3 to 1.5
- expert_gate: bfloat16 [32, 2048, 4096], P('sp', None, 'tp'), may hold values from -0.125 to 0.125
- expert_up: bfloat16 [32, 2048, 4096], P('sp', None, 'tp'), may hold values from -0.125 to 0.125
- expert_down: bfloat16 [32, 4096, 2048], P('sp', 'tp'), may hold values from -0.09375 to 0.09375
Outputs:
- layer_out: bfloat16 [8192, 2048], P('sp', 'tp')
The draws below stay inside these ranges and needn't reach their ends.
Inputs may be any that keep to these rules, and one draw needn't show every extreme that they name: `route_ids`: in each aligned block of 256 rows no expert is named by more than 32 rows; some expert is named by exactly 32 rows in some blocks.
All inputs are finite; a program needn't handle non-finite values.
Results may differ from the reference program's by a relative error of at most 0.017.
Values may be sent and summed in bfloat16 or wider, within the bound.
A program may use at most 64 MiB of HBM per device.

```python
import math
from functools import partial
import jax
import jax.numpy as jnp
import numpy as np
from jax import lax

D = 2048
CH = 1024
KW = 31
EXPERT_FF = 4096
TOP_K = 2
TOK_DEV = 256
TOKENS = 8192
EXPERTS = 32
CAP = 32
N_SP = 32
N_TP = 16


def draw_conv_value(key, part):
    spread = jnp.exp(jnp.log(6.0) * jnp.arange(CH, dtype=jnp.float32) / CH)
    sample = jnp.clip(jax.random.normal(key, (TOKENS, CH), jnp.float32), -5.0, 5.0)
    return (0.5 * sample * spread[None, :]).astype(jnp.bfloat16)


def levels(stream_key, dims, cuts, low, largest):
    def one(dim, blocks):
        steps = jax.random.uniform(jax.random.fold_in(jax.random.fold_in(stream_key, 6), dim), (blocks,), jnp.float32, low / len(cuts), largest / len(cuts))
        return jnp.repeat(jnp.exp(steps), dims[dim] // blocks).reshape((-1,) + (1,) * (len(dims) - dim - 1))

    level = one(*cuts[0])
    for cut in cuts[1:]:
        level = level * one(*cut)
    return level


def routed_block(own_key, own, number, rows, amount, top, bound, lean):
    order = jax.random.permutation(own_key, amount)
    crowded, usual = load_shares(amount, rows * top, bound, lean, True), load_shares(amount, rows * top, bound, lean, False)
    places = jnp.arange(amount)

    def named(lengths, turn):
        used = int((lengths > 0).sum())
        fixed = max(1, used // 4)
        moved = fixed + (places - fixed + turn * (used - fixed)) % max(1, amount - fixed)
        return jnp.zeros((amount,), jnp.int32).at[order[jnp.where(places < fixed, places, moved)]].set(jnp.asarray(lengths, jnp.int32))

    lengths = jnp.where(number % 4 == 0, named(crowded, number // 4), named(usual, number - number // 4 - 1))
    mixed = jax.random.permutation(jax.random.fold_in(own, 3), amount)
    source_of, receiver = mixed[0:amount // 2 * 2:2], mixed[1:amount // 2 * 2:2]
    room = jnp.minimum(lengths[source_of] - 1, bound - lengths[receiver]) // 2
    room = jnp.where((source_of == order[0]) | (receiver == order[0]) | (lengths[receiver] == 0), 0, jnp.maximum(room, 0))
    moved = jax.random.randint(jax.random.fold_in(own, 4), (amount // 2,), 0, 1 << 20) % (room + 1)
    lengths = lengths.at[source_of].add(-moved).at[receiver].add(moved)
    members = jnp.searchsorted(jnp.cumsum(lengths), jnp.arange(rows * top), side="right").astype(jnp.int32)
    table = members.reshape(top, rows).T
    table = table[jax.random.permutation(jax.random.fold_in(own, 1), rows)]
    turn = jax.random.randint(jax.random.fold_in(own, 2), (rows, 1), 0, top)
    return jnp.take_along_axis(table, (jnp.arange(top)[None, :] + turn) % top, axis=1)


def load_shares(count, total, bound, lean, full):
    portions = [(1 << 20) // math.isqrt(standing ** lean) + 1 for standing in range(1, count + 1)]
    largest = bound if full else min(bound, max(-(-total // count), total * portions[0] // sum(portions)))
    least = 1 if total - largest >= count - 1 else 0
    given, rest = [largest] + [least] * (count - 1), total - largest - least * (count - 1)
    while rest > 0:
        free = [i for i in range(1, count) if given[i] < largest] or [i for i in range(1, count) if given[i] < bound]
        whole, budget = sum([portions[i] for i in free]), rest
        for i in free:
            addition = min(bound - given[i], max(1, budget * portions[i] // whole), rest)
            given[i] = given[i] + addition
            rest = rest - addition
    return np.array(given)


def gaussian(stream_key, shape, width, most, split=(), held_as=jnp.bfloat16):
    array = width * jax.random.normal(stream_key, shape, jnp.float32)
    if split:
        array = array * levels(stream_key, shape, split, -0.22, 0.18)
    return jnp.clip(array, -most, most).astype(held_as)


def setup_inputs(seed: int = 0) -> dict:
    key_of = jax.random.split(jax.random.key(seed), 12)
    conv_value = draw_conv_value(jax.random.fold_in(key_of[11], 71), 0)
    conv_gate = gaussian(key_of[1], (TOKENS, CH), 1.5, 8.0, ((0, 32), (1, 16)))
    conv_taps = gaussian(key_of[2], (KW, CH), KW ** -0.5, 1.0, ((1, 16),))
    conv_gain = jnp.clip(1.0 + 0.18 * jax.random.normal(key_of[3], (CH,), jnp.float32), 0.1, 1.9)
    out_weight = gaussian(key_of[4], (CH, D), CH ** -0.5, 0.1875, ((0, 16),))
    residual = gaussian(key_of[5], (TOKENS, D), 1.0, 6.0, ((0, 32),))
    route_ids_keys = jax.random.split(jax.random.fold_in(key_of[6], 1), TOKENS // TOK_DEV)
    route_ids_turns = jax.random.permutation(jax.random.fold_in(key_of[6], 3), TOKENS // TOK_DEV)
    route_ids = jax.vmap(lambda own, number: routed_block(jax.random.fold_in(key_of[6], 2), own, number, TOK_DEV, EXPERTS, TOP_K, CAP, 2))(route_ids_keys, route_ids_turns).reshape((TOKENS, TOP_K))
    route_weight = jnp.clip(jnp.exp(math.log(1.5) - 1.60943787 * jax.random.uniform(key_of[7], (TOKENS, TOP_K), jnp.float32) ** levels(key_of[7], (TOKENS, TOP_K), ((0, 32),), -0.2, 0.2)), 0.3, 1.5)
    expert_gate = gaussian(key_of[8], (EXPERTS, D, EXPERT_FF), D ** -0.5, 0.125, ((0, 32), (2, 16)))
    expert_up = gaussian(key_of[9], (EXPERTS, D, EXPERT_FF), D ** -0.5, 0.125, ((0, 32), (2, 16)))
    expert_down = gaussian(key_of[10], (EXPERTS, EXPERT_FF, D), EXPERT_FF ** -0.5, 0.09375, ((0, 32), (1, 16)))
    return {"conv_value": conv_value, "conv_gate": conv_gate, "conv_taps": conv_taps, "conv_gain": conv_gain, "out_weight": out_weight, "residual": residual, "route_ids": route_ids, "route_weight": route_weight, "expert_gate": expert_gate, "expert_up": expert_up, "expert_down": expert_down}


def slot_plan(block_ids, experts, capacity):
    assigned = block_ids.reshape(-1)
    pair_count = assigned.shape[0]
    onehot = (assigned[:, None] == jnp.arange(experts, dtype=jnp.int32)[None, :]).astype(jnp.int32)
    earlier = jnp.cumsum(onehot, axis=0) - onehot
    ranking = lax.optimization_barrier(jnp.sum(earlier * onehot, axis=1))
    target = assigned * capacity + ranking
    owners = jnp.arange(pair_count, dtype=jnp.int32) // block_ids.shape[1]
    matches = target[None, :] == jnp.arange(experts * capacity, dtype=jnp.int32)[:, None]
    holder = lax.optimization_barrier(jnp.sum(jnp.where(matches, owners[None, :] + 1, 0), axis=1)) - 1
    holder = jnp.where(holder < 0, block_ids.shape[0], holder)
    return (target.astype(jnp.int32), holder.astype(jnp.int32))

def reference(conv_value, conv_gate, conv_taps, conv_gain, out_weight, residual, route_ids, route_weight, expert_gate, expert_up, expert_down):
    gated = conv_value.astype(jnp.float32) * jax.nn.sigmoid(conv_gate.astype(jnp.float32))
    padded = jnp.pad(gated, ((KW - 1, 0), (0, 0)))
    filtered = jnp.zeros((TOKENS, CH), jnp.float32)
    for offset in range(KW):
        filtered = filtered + conv_taps[offset].astype(jnp.float32) * padded[offset:offset + TOKENS]
    average = lax.optimization_barrier(jnp.mean(filtered, axis=1, keepdims=True))
    variance = lax.optimization_barrier(jnp.mean(filtered * filtered, axis=1, keepdims=True)) - average * average
    normed = (filtered - average) * lax.rsqrt(variance + 1e-05) * conv_gain.astype(jnp.float32)
    activated = jax.nn.silu(normed).astype(jnp.bfloat16)
    group_width = CH // N_TP
    mixed = jnp.zeros((TOKENS, D), jnp.float32)
    for group in range(N_TP):
        product = jnp.dot(activated[:, group * group_width:(group + 1) * group_width], out_weight[group * group_width:(group + 1) * group_width], preferred_element_type=jnp.float32)
        mixed = mixed + lax.optimization_barrier(product.astype(jnp.bfloat16)).astype(jnp.float32)
    updated = residual.astype(jnp.float32) + mixed
    normal_rows = (updated * lax.rsqrt(lax.optimization_barrier(jnp.mean(updated * updated, axis=1, keepdims=True)) + 1e-06)).astype(jnp.bfloat16)
    row_blocks = normal_rows.reshape(N_SP, TOK_DEV, D)
    id_blocks = route_ids.reshape(N_SP, TOK_DEV, TOP_K)
    targets, holders = jax.vmap(partial(slot_plan, experts=EXPERTS, capacity=CAP))(id_blocks)
    padded_rows = jnp.concatenate([row_blocks, jnp.zeros((N_SP, 1, D), jnp.bfloat16)], axis=1)
    expert_in = jnp.take_along_axis(padded_rows, holders[:, :, None], axis=1)
    expert_in = jnp.moveaxis(expert_in.reshape(N_SP, EXPERTS, CAP, D), 1, 0).reshape(EXPERTS, N_SP * CAP, D)
    hidden_group = EXPERT_FF // N_TP

    def one_expert(packed):
        rows_in, w_gate, w_up, w_down = packed
        gate_act = jnp.dot(rows_in, w_gate, preferred_element_type=jnp.float32)
        up_act = jnp.dot(rows_in, w_up, preferred_element_type=jnp.float32)
        hidden = (jax.nn.silu(gate_act) * up_act).astype(jnp.bfloat16)
        split_hidden = hidden.reshape(-1, N_TP, hidden_group).astype(jnp.float32)
        split_down = w_down.reshape(N_TP, hidden_group, D).astype(jnp.float32)
        pieces = jnp.einsum('rgf,gfd->grd', split_hidden, split_down)
        pieces = lax.optimization_barrier(pieces.astype(jnp.bfloat16)).astype(jnp.float32)
        return lax.optimization_barrier(jnp.sum(pieces, axis=0)).astype(jnp.bfloat16)
    expert_out = lax.map(one_expert, (expert_in, expert_gate, expert_up, expert_down))
    returned = jnp.moveaxis(expert_out.reshape(EXPERTS, N_SP, CAP, D), 1, 0).reshape(N_SP, EXPERTS * CAP, D)
    picked = jnp.take_along_axis(returned, targets[:, :, None], axis=1).reshape(TOKENS, TOP_K, D)
    combined = lax.optimization_barrier(jnp.sum(picked.astype(jnp.float32) * route_weight[:, :, None], axis=1))
    return (updated + combined).astype(jnp.bfloat16)
```

```python
import functools

import jax
import jax.numpy as jnp
from jax import lax
from jax.experimental import pallas as pl
from jax.experimental.pallas import tpu as pltpu
from jax.sharding import PartitionSpec as P

MESH = pl.DeviceIdType.MESH
F32, BF16 = jnp.float32, jnp.bfloat16
HALO = 32
ORDER = (0, 4, 1, 5, 2, 6, 3, 7)


def iota(shape, dim):
    return lax.broadcasted_iota(jnp.int32, shape, dim)


def matmul(a, b, precision=None):
    return jnp.dot(a, b, preferred_element_type=F32, precision=precision)


def layer(
    n_sp, n_y,
    cv, cg, taps, gain, ow, res, ids, rw, eg, eu, ed,
    out,
    pk_own, pk_par, tg_own, tg_par, gext, stats, actb, wc, resv, upd, ub, a0s, a1s, gs,
    gath, rows, wgu, wd, acc, ssq, hid, pbuf, sbuf, rbuf, eo, back, xs, xr,
    l_sem, sw_s, sw_r, h_s, h_r, w_s, w_r, st_s, st_r, a_s, a_r, d_s, d_r, g_s, g_r, r_s, r_r,
    b_s, b_r,
):
    sp, tp = lax.axis_index("sp"), lax.axis_index("tp")
    y, c = tp // 2, tp % 2
    other = 1 - c
    partner = (sp, y * 2 + other)
    tok, ch = cv.shape
    half = tok // 2
    width = res.shape[1]
    cols = width // n_y
    ff = eg.shape[2]
    slots = gath.shape[0]
    per = slots // n_sp
    part = slots // 8
    mid = slots // 2

    def column(k):
        return (sp, lax.rem(y + k, n_y) * 2 + c)

    def plane(k):
        return (lax.rem(sp + k, n_sp), tp)

    def remote(src, dst, s, r, dev):
        return pltpu.make_async_remote_copy(
            src_ref=src, dst_ref=dst, send_sem=s, recv_sem=r, device_id=dev, device_id_type=MESH
        )

    my_cols = pl.ds(pl.multiple_of(y * cols, cols), cols)
    my_half = pl.ds(pl.multiple_of(c * half, half), half)
    loads = [
        pltpu.make_async_copy(res.at[my_half, my_cols], resv, l_sem.at[0]),
        pltpu.make_async_copy(eg.at[0], wgu.at[0], l_sem.at[1]),
        pltpu.make_async_copy(eu.at[0], wgu.at[2], l_sem.at[2]),
        pltpu.make_async_copy(ed.at[0], wd.at[pl.ds(0, ff)], l_sem.at[3]),
        pltpu.make_async_copy(
            ow.at[:, my_cols],
            wc.at[y, pl.ds(pl.multiple_of(c * ch, ch), ch)],
            l_sem.at[4],
        ),
    ]
    for load in loads:
        load.start()

    barrier = pltpu.get_barrier_semaphore()

    def greet(dev):
        pl.semaphore_signal(barrier, inc=1, device_id=dev, device_id_type=MESH)

    greet(partner)
    nxt = lax.rem(sp + 1, n_sp)
    prv = lax.rem(sp + n_sp - 1, n_sp)
    greet((nxt, y * 2 + other))
    greet((prv, y * 2 + other))

    @pl.loop(1, n_y)
    def _(k):
        greet(column(k))

    @pl.loop(1, n_sp)
    def _(k):
        greet(plane(k))

    lane = iota((ch, 2 * ch), 1)
    chan = iota((ch, 2 * ch), 0)
    put_low = (lane == chan).astype(BF16)
    put_high = (lane == chan + ch).astype(BF16)
    pk_own[pl.ds(HALO, tok), :] = (matmul(cv[...], put_low) + matmul(cg[...], put_high)).astype(BF16)
    n_taps = taps.shape[0]
    tg_own[...] = jnp.zeros_like(tg_own)
    tg_own[pl.ds(0, n_taps), :] = matmul(taps[...], put_low)
    tg_own[pl.ds(n_taps, 1), :] = matmul(
        jnp.broadcast_to(gain[...], (8, ch)), put_low.astype(F32), lax.Precision.HIGHEST
    )[0:1]

    pl.semaphore_wait(barrier, 3 + (n_y - 1) + (n_sp - 1))

    body = pl.ds(HALO, tok)
    head = pl.ds(0, HALO)
    tail = pl.ds(tok, HALO)
    halo = [
        remote(pk_own.at[tail], pk_own.at[head], h_s.at[0], h_r.at[0], (nxt, tp)),
        remote(pk_own.at[tail], pk_par.at[head], h_s.at[1], h_r.at[1], (nxt, y * 2 + other)),
    ]
    for copy in halo:
        copy.start()
    swap_pk = remote(pk_own.at[body], pk_par.at[body], sw_s.at[0], sw_r.at[0], partner)
    swap_tg = remote(tg_own, tg_par, sw_s.at[1], sw_r.at[1], partner)
    swap_pk.start()
    swap_tg.start()

    def wc_copy(k):
        far = lax.rem(y + k, n_y)
        return remote(
            ow.at[:, pl.ds(pl.multiple_of(far * cols, cols), cols)],
            wc.at[y, pl.ds(pl.multiple_of(c * ch, ch), ch)],
            w_s,
            w_r.at[y],
            column(k),
        )

    @pl.loop(1, n_y)
    def _(k):
        wc_copy(k).start()

    swap_w = [
        remote(eg.at[0], wgu.at[1], sw_s.at[2], sw_r.at[2], partner),
        remote(eu.at[0], wgu.at[3], sw_s.at[3], sw_r.at[3], partner),
        remote(ed.at[0], wd.at[pl.ds(ff, ff)], sw_s.at[4], sw_r.at[4], partner),
    ]
    for copy in swap_w:
        copy.start()

    expert = iota((tok, 128), 1)
    id0, id1 = ids[:, 0:1], ids[:, 1:2]
    hot0, hot1 = (id0 == expert).astype(F32), (id1 == expert).astype(F32)
    before = (iota((tok, tok), 1) < iota((tok, tok), 0)).astype(BF16)
    earlier = matmul(before, (hot0 + hot1).astype(BF16))

    def slot_of(ident, hot):
        rank = jnp.sum(earlier * hot, axis=1, keepdims=True).astype(jnp.int32) - c * per
        return jnp.where((rank >= 0) & (rank < per), ident * per + rank, -1)

    slot0, slot1 = slot_of(id0, hot0), slot_of(id1, hot1)
    place = iota((tok, slots), 1)
    a0s[...] = (place == slot0).astype(BF16)
    a1s[...] = (place == slot1).astype(BF16)

    def along(v):
        return jnp.transpose(jnp.broadcast_to(v.astype(F32), (tok, 128)))[0:1, :]

    row0, row1 = along(slot0), along(slot1)
    place_row = iota((slots, tok), 0).astype(F32)
    gs[...] = jnp.where((place_row == row0) | (place_row == row1), 1.0, 0.0).astype(BF16)

    swap_tg.wait_recv()
    swap_pk.wait_recv()
    for copy in halo:
        copy.wait_recv()
    wide = 2 * ch
    lane2, chan2 = iota((wide, wide), 1), iota((wide, wide), 0)

    def pick(first, to):
        return ((chan2 >= first) & (chan2 < first + ch) & (lane2 == chan2 - first + to * ch)).astype(BF16)

    span = pl.ds(pl.multiple_of(c * half, half), half + HALO)
    mine, theirs = pk_own[span, :], pk_par[span, :]
    value = matmul(mine, pick(0, c)) + matmul(theirs, pick(0, other))
    gate = matmul(mine, pick(ch, c)) + matmul(theirs, pick(ch, other))
    gated = value / (1.0 + jnp.exp(-gate))
    start = (iota(gated.shape, 0) < HALO) & (sp == 0) & (c == 0)
    gext[...] = jnp.where(start, 0.0, gated)
    tg = matmul(tg_own[...], pick(0, c).astype(F32), lax.Precision.HIGHEST) + matmul(
        tg_par[...], pick(0, other).astype(F32), lax.Precision.HIGHEST
    )
    filtered = jnp.zeros((half, wide), F32)
    for i in range(n_taps):
        filtered = filtered + tg[i : i + 1, :] * gext[pl.ds(i + HALO + 1 - n_taps, half), :]

    turned = jnp.transpose(filtered)
    sums = jnp.sum(turned, axis=0, keepdims=True)
    squares = jnp.sum(turned * turned, axis=0, keepdims=True)
    stats[y] = jnp.where(iota((8, half), 0) == 0, sums, squares)

    def st_copy(k):
        return remote(stats.at[y], stats.at[y], st_s, st_r.at[y], column(k))

    @pl.loop(1, n_y)
    def _(k):
        st_copy(k).start()

    @pl.loop(1, n_y)
    def _(k):
        origin = lax.rem(y + k, n_y)
        remote(stats.at[origin], stats.at[origin], st_s, st_r.at[origin], column(k)).wait_recv()

    total = stats[0]
    for o in range(1, n_y):
        total = total + stats[o]
    total = total / (n_y * wide)
    average, power = total[0:1, :], total[1:2, :]
    scale = lax.rsqrt(power - average * average + 1e-05)

    def down(v):
        return jnp.transpose(jnp.broadcast_to(v, (wide, half)))

    normed = (filtered - down(average)) * down(scale) * tg[n_taps : n_taps + 1, :]
    actb[y] = (normed / (1.0 + jnp.exp(-normed))).astype(BF16)

    def a_copy(k):
        return remote(actb.at[y], actb.at[y], a_s, a_r.at[y], column(k))

    @pl.loop(1, n_y)
    def _(k):
        a_copy(k).start()

    own_rows = pl.ds(pl.multiple_of(c * ch, ch), ch)
    loads[4].wait()

    @pl.loop(1, n_y)
    def _(k):
        origin = lax.rem(y + k, n_y)
        remote(
            wc.at[origin, own_rows], wc.at[origin, own_rows], w_s, w_r.at[origin], column(k)
        ).wait_recv()

    swap_wc = remote(wc.at[:, own_rows], wc.at[:, own_rows], sw_s.at[5], sw_r.at[5], partner)
    swap_wc.start()
    loads[0].wait()
    swap_wc.wait_recv()
    upd[...] = resv[...].astype(F32) + matmul(actb[y], wc[y])

    @pl.loop(1, n_y)
    def _(k):
        origin = lax.rem(y + k, n_y)
        remote(actb.at[origin], actb.at[origin], a_s, a_r.at[origin], column(k)).wait_recv()
        upd[...] += matmul(actb[origin], wc[origin])

    ub[my_half, :] = upd[...].astype(BF16)
    swap_ub = remote(ub.at[my_half], ub.at[my_half], sw_s.at[6], sw_r.at[6], partner)
    swap_ub.start()
    swap_ub.wait_recv()

    gath[...] = matmul(gs[...], ub[...]).astype(BF16)

    def at(k):
        return pl.ds(pl.multiple_of(k * per, per), per)

    @pl.loop(1, n_sp)
    def _(k):
        dst = lax.rem(sp + k, n_sp)
        remote(gath.at[at(dst)], rows.at[y, at(sp)], d_s, d_r.at[sp], plane(k)).start()

    keep = pltpu.make_async_copy(gath.at[at(sp)], rows.at[y, at(sp)], d_r.at[sp])
    keep.start()

    for load in loads[1:4]:
        load.wait()
    for copy in swap_w:
        copy.wait_recv()

    def stream(q):
        return pl.ds(q * part, part)

    def turn(q):
        return 1 if q < 4 else -1

    def ring_copy(step, q):
        origin = lax.rem(y + n_y - turn(q) * step, n_y)
        return remote(
            rows.at[origin, stream(q)], rows.at[origin, stream(q)], g_s, g_r.at[step, q],
            column(turn(q) + n_y),
        )

    for q in ORDER:
        for k in range(q * part // per, (q + 1) * part // per):
            pltpu.make_async_copy(rows.at[y, at(k)], rows.at[y, at(k)], d_r.at[k]).wait()
        ring_copy(0, q).start()

    acc[...] = jnp.zeros_like(acc)
    ssq[...] = jnp.zeros_like(ssq)

    def accumulate(origin, first):
        block = pl.ds(first, mid)
        x = rows[origin, block, :]
        xf = x.astype(F32)
        xf = xf * xf
        folded = xf[:, 0:128]
        for j in range(1, cols // 128):
            folded = folded + xf[:, j * 128 : (j + 1) * 128]
        ssq[block, :] += folded
        deep = pl.ds(pl.multiple_of(origin * cols, cols), cols)
        for j in range(4):
            acc[j, block, :] += matmul(x, wgu[j, deep, :])

    accumulate(y, 0)
    accumulate(y, mid)

    @pl.loop(0, n_y - 1)
    def _(step):
        for q in ORDER:
            ring_copy(step, q).wait_recv()

            @pl.when(step < n_y - 2)
            def _():
                ring_copy(step + 1, q).start()

        accumulate(lax.rem(y + n_y - 1 - step, n_y), 0)
        accumulate(lax.rem(y + 1 + step, n_y), mid)

    rms = lax.rsqrt(jnp.sum(ssq[...], axis=1, keepdims=True) / width + 1e-06)
    for j in range(2):
        g = acc[j] * rms
        u = acc[2 + j] * rms
        hid[:, j * ff : (j + 1) * ff] = (g / (1.0 + jnp.exp(-g)) * u).astype(BF16)

    def product(first, chunk):
        block = pl.ds(first, mid)
        at_cols = pl.ds(pl.multiple_of(chunk * cols, cols), cols)
        pbuf[block, :] = matmul(hid[block, :], wd[:, at_cols])

    def sum_copy(step, q):
        return remote(
            sbuf.at[step, stream(q)], rbuf.at[step, stream(q)], r_s, r_r.at[step, q],
            column(turn(q) + n_y),
        )

    product(0, lax.rem(y + n_y - 1, n_y))
    product(mid, lax.rem(y + 1, n_y))
    for q in ORDER:
        sbuf[0, stream(q), :] = pbuf[stream(q), :].astype(BF16)
        sum_copy(0, q).start()

    @pl.loop(1, n_y - 1)
    def _(step):
        product(0, lax.rem(y + n_y - 1 - step, n_y))
        product(mid, lax.rem(y + 1 + step, n_y))
        for q in ORDER:
            sum_copy(step - 1, q).wait_recv()
            both = pbuf[stream(q), :] + rbuf[step - 1, stream(q), :].astype(F32)
            sbuf[step, stream(q), :] = both.astype(BF16)
            sum_copy(step, q).start()

    product(0, y)
    product(mid, y)

    def back_copy(dst):
        return remote(eo.at[at(dst)], back.at[at(sp)], b_s, b_r, (dst, tp))

    for q in ORDER:
        sum_copy(n_y - 2, q).wait_recv()
        both = pbuf[stream(q), :] + rbuf[n_y - 2, stream(q), :].astype(F32)
        eo[stream(q), :] = both.astype(BF16)
        for k in range(q * part // per, (q + 1) * part // per):

            @pl.when(sp != k)
            def _():
                back_copy(jnp.int32(k)).start()

    stay = pltpu.make_async_copy(eo.at[at(sp)], back.at[at(sp)], l_sem.at[5])
    stay.start()
    stay.wait()
    most = pl.ds(0, slots - per)
    pltpu.make_async_copy(back.at[most], back.at[most], b_r).wait()

    w0, w1 = rw[:, 0:1], rw[:, 1:2]
    combined = w0 * matmul(a0s[...], back[...]) + w1 * matmul(a1s[...], back[...])
    xs[0] = combined[:, 0 : cols // 2]
    xs[1] = combined[:, cols // 2 :]
    xs[0, my_half, :] += upd[:, 0 : cols // 2]
    xs[1, my_half, :] += upd[:, cols // 2 :]
    last = remote(xs.at[other], xr, sw_s.at[7], sw_r.at[7], partner)
    last.start()
    last.wait_recv()
    out[...] = (xs[c] + xr[...]).astype(BF16)

    for copy in halo + swap_w + [swap_pk, swap_tg, swap_wc, swap_ub, last]:
        copy.wait_send()
    many = pl.ds(0, n_y - 1)
    pltpu.make_async_copy(wc.at[many, own_rows], wc.at[many, own_rows], w_s).wait()
    pltpu.make_async_copy(stats.at[many], stats.at[many], st_s).wait()
    pltpu.make_async_copy(actb.at[many], actb.at[many], a_s).wait()
    pltpu.make_async_copy(gath.at[most], gath.at[most], d_s).wait()
    pltpu.make_async_copy(rows.at[many], rows.at[many], g_s).wait()
    pltpu.make_async_copy(sbuf, sbuf, r_s).wait()
    pltpu.make_async_copy(eo.at[most], eo.at[most], b_s).wait()


def solution(mesh):
    n_sp, n_y = mesh.shape["sp"], mesh.shape["tp"] // 2

    def local(cv, cg, taps, gain, ow, res, ids, rw, eg, eu, ed):
        tok, ch = cv.shape
        width = res.shape[1]
        cols = width // n_y
        ff = eg.shape[2]
        slots = tok * ids.shape[1]
        half = tok // 2
        vm, hbm = pl.BlockSpec(memory_space=pltpu.VMEM), pl.BlockSpec(memory_space=pl.ANY)
        dma = pltpu.SemaphoreType.DMA
        scratch = [
            pltpu.VMEM((HALO + tok, 2 * ch), BF16),
            pltpu.VMEM((HALO + tok, 2 * ch), BF16),
            pltpu.VMEM((40, 2 * ch), F32),
            pltpu.VMEM((40, 2 * ch), F32),
            pltpu.VMEM((HALO + half, 2 * ch), F32),
            pltpu.VMEM((n_y, 8, half), F32),
            pltpu.VMEM((n_y, half, 2 * ch), BF16),
            pltpu.VMEM((n_y, 2 * ch, cols), BF16),
            pltpu.VMEM((half, cols), BF16),
            pltpu.VMEM((half, cols), F32),
            pltpu.VMEM((tok, cols), BF16),
            pltpu.VMEM((tok, slots), BF16),
            pltpu.VMEM((tok, slots), BF16),
            pltpu.VMEM((slots, tok), BF16),
            pltpu.VMEM((slots, cols), BF16),
            pltpu.VMEM((n_y, slots, cols), BF16),
            pltpu.VMEM((4, width, ff), BF16),
            pltpu.VMEM((2 * ff, width), BF16),
            pltpu.VMEM((4, slots, ff), F32),
            pltpu.VMEM((slots, 128), F32),
            pltpu.VMEM((slots, 2 * ff), BF16),
            pltpu.VMEM((slots, cols), F32),
            pltpu.VMEM((n_y - 1, slots, cols), BF16),
            pltpu.VMEM((n_y - 1, slots, cols), BF16),
            pltpu.VMEM((slots, cols), BF16),
            pltpu.VMEM((slots, cols), BF16),
            pltpu.VMEM((2, tok, cols // 2), F32),
            pltpu.VMEM((tok, cols // 2), F32),
            dma((6,)), dma((8,)), dma((8,)), dma((2,)), dma((2,)),
            dma, dma((n_y,)), dma, dma((n_y,)), dma, dma((n_y,)),
            dma, dma((n_sp,)), dma, dma((n_y - 1, 8)), dma, dma((n_y - 1, 8)),
            dma, dma,
        ]
        return pl.pallas_call(
            functools.partial(layer, n_sp, n_y),
            out_shape=jax.ShapeDtypeStruct((tok, cols // 2), BF16),
            in_specs=[vm, vm, vm, vm, hbm, hbm, vm, vm, hbm, hbm, hbm],
            out_specs=vm,
            scratch_shapes=scratch,
            compiler_params=pltpu.CompilerParams(
                collective_id=0, has_side_effects=True, vmem_limit_bytes=56 << 20
            ),
        )(cv, cg, taps, gain.reshape(1, ch), ow, res, ids, rw, eg, eu, ed)

    placed = (
        P("sp", "tp"), P("sp", "tp"), P(None, "tp"), P("tp"), P("tp", None), P("sp", None),
        P("sp", None), P("sp", None), P("sp", None, "tp"), P("sp", None, "tp"), P("sp", "tp", None),
    )
    return jax.shard_map(local, mesh=mesh, in_specs=placed, out_specs=P("sp", "tp"), check_vma=False)
```

```python
import functools

import jax
import jax.numpy as jnp
from jax import lax
from jax.experimental import pallas as pl
from jax.experimental.pallas import tpu as pltpu
from jax.sharding import PartitionSpec as P

MESH = pl.DeviceIdType.MESH
F32, BF16 = jnp.float32, jnp.bfloat16
HALO = 32
STREAMS = 8
PAIRS = ((0, 7), (1, 6), (2, 5), (3, 4))
ORDER = (0, 7, 1, 6, 2, 5, 3, 4)


def iota(shape, dim):
    return lax.broadcasted_iota(jnp.int32, shape, dim)


def matmul(a, b, precision=None):
    return jnp.dot(a, b, preferred_element_type=F32, precision=precision)


def matmul_t(a, b):
    return lax.dot_general(a, b, (((0,), (0,)), ((), ())), preferred_element_type=F32)


def layer(
    n_sp, n_y,
    cv, cg, taps, gain, ow, res, ids, rw, eg, eu, ed,
    out,
    pk_own, pk_par, tg_own, tg_par, gext, stats, gains, gcol, devs, wc, resv, upd, ub, gs, wts,
    gath, rows, wgu, wd, acc, ssq, hid, sbuf, rbuf, eo, back, xs, xr,
    l_sem, sw_s, sw_r, h_s, h_r, w_s, w_r, st_s, st_r, a_s, a_r, gn_s, gn_r, d_s, d_r, g_s, g_r,
    r_s, r_r, b_s, b_r,
):
    sp, tp = lax.axis_index("sp"), lax.axis_index("tp")
    y, c = tp // 2, tp % 2
    other = 1 - c
    n_x = n_sp // STREAMS
    z, x = sp // n_x, sp % n_x
    partner = (sp, y * 2 + other)
    ch, tok = cv.shape
    half = tok // 2
    wide = 2 * ch
    width = res.shape[1]
    cols = width // n_y
    ff = eg.shape[2]
    slots = gath.shape[0]
    per = slots // n_sp
    part = slots // STREAMS
    mid = slots // 2

    def column(k):
        return (sp, lax.rem(y + k, n_y) * 2 + c)

    def remote(src, dst, s, r, dev):
        return pltpu.make_async_remote_copy(
            src_ref=src, dst_ref=dst, send_sem=s, recv_sem=r, device_id=dev, device_id_type=MESH
        )

    my_cols = pl.ds(pl.multiple_of(y * cols, cols), cols)
    my_half = pl.ds(pl.multiple_of(c * half, half), half)
    own_rows = pl.ds(pl.multiple_of(c * ch, ch), ch)
    loads = [
        pltpu.make_async_copy(res.at[my_half, my_cols], resv, l_sem.at[0]),
        pltpu.make_async_copy(eg.at[0], wgu.at[0], l_sem.at[1]),
        pltpu.make_async_copy(eu.at[0], wgu.at[2], l_sem.at[2]),
        pltpu.make_async_copy(ed.at[0], wd.at[pl.ds(0, ff)], l_sem.at[3]),
        pltpu.make_async_copy(ow.at[:, my_cols], wc.at[y, own_rows], l_sem.at[4]),
    ]
    for load in loads:
        load.start()

    barrier = pltpu.get_barrier_semaphore()

    def greet(dev):
        pl.semaphore_signal(barrier, inc=1, device_id=dev, device_id_type=MESH)

    nxt = lax.rem(sp + 1, n_sp)
    prv = lax.rem(sp + n_sp - 1, n_sp)

    @pl.loop(1, n_sp)
    def _(k):
        greet((lax.rem(sp + k, n_sp), tp))

    @pl.loop(1, n_y)
    def _(k):
        greet(column(k))

    greet((nxt, y * 2 + other))
    greet((prv, y * 2 + other))
    greet(partner)

    lane = iota((ch, wide), 1)
    chan = iota((ch, wide), 0)
    put_low = (lane == chan).astype(BF16)
    put_high = (lane == chan + ch).astype(BF16)
    pk_own[pl.ds(HALO, tok), :] = (
        matmul_t(cv[...], put_low) + matmul_t(cg[...], put_high)
    ).astype(BF16)
    n_taps = taps.shape[0]
    tg_own[...] = jnp.zeros_like(tg_own)
    tg_own[pl.ds(0, n_taps), :] = matmul(taps[...], put_low)
    tg_own[pl.ds(n_taps, 1), :] = matmul(
        jnp.broadcast_to(gain[...], (8, ch)), put_low.astype(F32), lax.Precision.HIGHEST
    )[0:1]

    expert = iota((128, tok), 0)
    id0, id1 = ids[0:1, :], ids[1:2, :]
    hot0, hot1 = (id0 == expert).astype(F32), (id1 == expert).astype(F32)
    before = (iota((tok, tok), 0) < iota((tok, tok), 1)).astype(BF16)
    earlier = matmul((hot0 + hot1).astype(BF16), before)
    place = iota((slots, tok), 0)
    for k, (ident, hot) in enumerate(((id0, hot0), (id1, hot1))):
        rank = jnp.sum(earlier * hot, axis=0, keepdims=True).astype(jnp.int32) - c * per
        slot = jnp.where((rank >= 0) & (rank < per), ident * per + rank, -1)
        gs[k] = jnp.where(place == slot, 1.0, 0.0).astype(BF16)
        wts[k] = jnp.transpose(jnp.broadcast_to(rw[k : k + 1, :], (128, tok)))

    pl.semaphore_wait(barrier, 3 + (n_y - 1) + (n_sp - 1))

    body = pl.ds(HALO, tok)
    head = pl.ds(0, HALO)
    tail = pl.ds(tok, HALO)
    halo = [
        remote(pk_own.at[tail], pk_own.at[head], h_s.at[0], h_r.at[0], (nxt, tp)),
        remote(pk_own.at[tail], pk_par.at[head], h_s.at[1], h_r.at[1], (nxt, y * 2 + other)),
    ]
    for copy in halo:
        copy.start()
    swap_tg = remote(tg_own, tg_par, sw_s.at[1], sw_r.at[1], partner)
    swap_pk = remote(pk_own.at[body], pk_par.at[body], sw_s.at[0], sw_r.at[0], partner)
    swap_tg.start()
    swap_pk.start()

    @pl.loop(1, n_y)
    def _(k):
        far = lax.rem(y + k, n_y)
        far_cols = pl.ds(pl.multiple_of(far * cols, cols), cols)
        remote(ow.at[:, far_cols], wc.at[y, own_rows], w_s, w_r.at[y], column(k)).start()

    swap_w = [
        remote(eg.at[0], wgu.at[1], sw_s.at[2], sw_r.at[2], partner),
        remote(eu.at[0], wgu.at[3], sw_s.at[3], sw_r.at[3], partner),
        remote(ed.at[0], wd.at[pl.ds(ff, ff)], sw_s.at[4], sw_r.at[4], partner),
    ]
    for copy in swap_w:
        copy.start()

    lane2, chan2 = iota((wide, wide), 1), iota((wide, wide), 0)

    def pick(first, to):
        return (
            (chan2 >= first) & (chan2 < first + ch) & (lane2 == chan2 - first + to * ch)
        ).astype(BF16)

    swap_tg.wait_recv()
    tg = matmul(tg_own[...], pick(0, c).astype(F32), lax.Precision.HIGHEST) + matmul(
        tg_par[...], pick(0, other).astype(F32), lax.Precision.HIGHEST
    )

    def everywhere(buf, s, r):
        @pl.loop(1, n_y)
        def _(k):
            remote(buf.at[y], buf.at[y], s, r.at[y], column(k)).start()

    def arrived(buf, s, r, k):
        origin = lax.rem(y + k, n_y)
        remote(buf.at[origin], buf.at[origin], s, r.at[origin], column(k)).wait_recv()
        return origin

    swap_pk.wait_recv()
    for copy in halo:
        copy.wait_recv()
    span = pl.ds(pl.multiple_of(c * half, half), half + HALO)
    mine, theirs = pk_own[span, :], pk_par[span, :]
    value = matmul(mine, pick(0, c)) + matmul(theirs, pick(0, other))
    gate = matmul(mine, pick(ch, c)) + matmul(theirs, pick(ch, other))
    gated = value / (1.0 + jnp.exp(-gate))
    start = (iota(gated.shape, 0) < HALO) & (sp == 0) & (c == 0)
    gext[...] = jnp.where(start, 0.0, gated)
    filtered = jnp.zeros((half, wide), F32)
    for i in range(n_taps):
        filtered = filtered + tg[i : i + 1, :] * gext[pl.ds(i + HALO + 1 - n_taps, half), :]

    turned = jnp.transpose(filtered)
    mean = jnp.sum(turned, axis=0, keepdims=True) / wide
    turned = turned - mean
    spread = jnp.sum(turned * turned, axis=0, keepdims=True) / wide
    devs[y] = turned.astype(BF16)
    stats[y] = jnp.where(iota((8, half), 0) == 0, mean, spread)
    gains[y] = jnp.broadcast_to(tg[n_taps : n_taps + 1, :], (8, wide))
    everywhere(stats, st_s, st_r)
    everywhere(gains, gn_s, gn_r)
    everywhere(devs, a_s, a_r)

    loads[4].wait()

    @pl.loop(1, n_y)
    def _(k):
        origin = lax.rem(y + k, n_y)
        remote(
            wc.at[origin, own_rows], wc.at[origin, own_rows], w_s, w_r.at[origin], column(k)
        ).wait_recv()

    swap_wc = remote(wc.at[:, own_rows], wc.at[:, own_rows], sw_s.at[5], sw_r.at[5], partner)
    swap_wc.start()

    @pl.loop(1, n_y)
    def _(k):
        arrived(stats, st_s, st_r, k)
        arrived(gains, gn_s, gn_r, k)

    average = stats[0, 0:1, :]
    for o in range(1, n_y):
        average = average + stats[o, 0:1, :]
    average = average / n_y
    variance = jnp.zeros_like(average)
    for o in range(n_y):
        gap = stats[o, 0:1, :] - average
        variance = variance + (stats[o, 1:2, :] + gap * gap)
    scale = lax.rsqrt(variance / n_y + 1e-05)
    for o in range(n_y):
        gcol[o] = jnp.transpose(jnp.broadcast_to(gains[o, 0:1, :], (half, wide))) * scale

    def mixed(origin):
        shift = stats[origin, 0:1, :] - average
        normed = (devs[origin].astype(F32) + shift) * gcol[origin]
        activated = (normed / (1.0 + jnp.exp(-normed))).astype(BF16)
        return matmul_t(activated, wc[origin])

    loads[0].wait()
    swap_wc.wait_recv()
    upd[...] = resv[...].astype(F32) + mixed(y)
    for k in (1, 7, 2, 6, 3, 5, 4) if n_y == 8 else range(1, n_y):
        upd[...] += mixed(arrived(devs, a_s, a_r, k))

    ub[my_half, :] = upd[...].astype(BF16)
    swap_ub = remote(ub.at[my_half], ub.at[my_half], sw_s.at[6], sw_r.at[6], partner)
    swap_ub.start()
    swap_ub.wait_recv()

    gath[...] = matmul(gs[0] + gs[1], ub[...]).astype(BF16)

    def at(k):
        return pl.ds(pl.multiple_of(k * per, per), per)

    def below(j):
        return lax.rem(z + STREAMS - j, STREAMS)

    def above(j):
        return lax.rem(z + j, STREAMS)

    for j in ORDER:
        spot = j * n_x + x
        for i in range(n_x):
            dst = below(j) * n_x + lax.rem(x + i, n_x)
            if i == 0 and j == 0:
                keep = pltpu.make_async_copy(gath.at[at(dst)], rows.at[y, at(spot)], d_r.at[spot])
                keep.start()
            else:
                remote(gath.at[at(dst)], rows.at[y, at(spot)], d_s, d_r.at[spot], (dst, tp)).start()

    for load in loads[1:4]:
        load.wait()
    for copy in swap_w:
        copy.wait_recv()
    acc[...] = jnp.zeros_like(acc)
    ssq[...] = jnp.zeros_like(ssq)

    def stream(j):
        return pl.ds(j * part, part)

    def turn(j):
        return 1 if j < STREAMS // 2 else -1

    def source(step, j):
        return lax.rem(y + n_y - turn(j) * step, n_y)

    def ring_copy(step, j):
        origin = source(step, j)
        return remote(
            rows.at[origin, stream(j)], rows.at[origin, stream(j)], g_s, g_r.at[step, j],
            column(turn(j) + n_y),
        )

    def deep(origin):
        return pl.ds(pl.multiple_of(origin * cols, cols), cols)

    def folded(v):
        v = v.astype(F32)
        v = v * v
        total = v[:, 0:128]
        for i in range(1, cols // 128):
            total = total + v[:, i * 128 : (i + 1) * 128]
        return total

    def accumulate(origin, block):
        v = rows[origin, block, :]
        ssq[block, :] += folded(v)
        for i in range(4):
            acc[i, block, :] += matmul(v, wgu[i, deep(origin), :])

    early = 4

    def finish(j):
        block = stream(j)
        for step in range(early + 1, n_y):
            accumulate(source(step, j), block)
        rms = lax.rsqrt(jnp.sum(ssq[block, :], axis=1, keepdims=True) / width + 1e-06)
        for i in range(2):
            g = acc[i, block, :] * rms
            u = acc[2 + i, block, :] * rms
            hid[block, i * ff : (i + 1) * ff] = (g / (1.0 + jnp.exp(-g)) * u).astype(BF16)

    def sum_copy(step, j):
        return remote(
            sbuf.at[step, stream(j)], rbuf.at[step, stream(j)], r_s, r_r.at[step, j],
            column(turn(j) + n_y),
        )

    def product(step, j):
        chunk = source(step + 1, j)
        return matmul(hid[stream(j), :], wd[:, pl.ds(pl.multiple_of(chunk * cols, cols), cols)])

    def send_sum(step, j):
        partial = product(step, j)
        if step > 0:
            sum_copy(step - 1, j).wait_recv()
            partial = partial + rbuf[step - 1, stream(j), :].astype(F32)
        sbuf[step, stream(j), :] = partial.astype(BF16)
        sum_copy(step, j).start()

    def send_back(j):
        partial = product(n_y - 1, j)
        sum_copy(n_y - 2, j).wait_recv()
        eo[stream(j), :] = (partial + rbuf[n_y - 2, stream(j), :].astype(F32)).astype(BF16)
        for i in range(n_x):
            spot = j * n_x + i
            dst = above(j) * n_x + i
            if j == 0:

                @pl.when(x != i)
                def _():
                    remote(eo.at[at(spot)], back.at[at(sp)], b_s, b_r, (dst, tp)).start()

            else:
                remote(eo.at[at(spot)], back.at[at(sp)], b_s, b_r, (dst, tp)).start()

    lag = len(PAIRS) - 1
    for t in range(-1, 2 * n_y + lag + 1):
        for i, pair in enumerate(PAIRS):
            step = t - i
            for j in pair:
                if step == -1:
                    for k in range(j * n_x, (j + 1) * n_x):
                        spot = rows.at[y, at(k)]
                        pltpu.make_async_copy(spot, spot, d_r.at[k]).wait()
                    ring_copy(0, j).start()
                elif 0 <= step < n_y - 1:
                    ring_copy(step, j).wait_recv()
                    if step < n_y - 2:
                        ring_copy(step + 1, j).start()
        done = t - lag + 1
        if 0 <= done <= early:
            accumulate(source(done, 0), pl.ds(0, mid))
            accumulate(source(done, STREAMS - 1), pl.ds(mid, mid))
        for i, pair in enumerate(PAIRS):
            step = t - i - (n_y - 2)
            for j in pair:
                if step == 0:
                    finish(j)
                if 0 <= step < n_y - 1:
                    send_sum(step, j)
                elif step == n_y - 1:
                    send_back(j)

    stay = pltpu.make_async_copy(eo.at[at(x)], back.at[at(sp)], l_sem.at[5])
    stay.start()
    stay.wait()
    most = pl.ds(0, slots - per)
    pltpu.make_async_copy(back.at[most], back.at[most], b_r).wait()

    first, second = matmul_t(gs[0], back[...]), matmul_t(gs[1], back[...])
    for i in range(2):
        lanes = slice(i * (cols // 2), (i + 1) * (cols // 2))
        xs[i] = wts[0] * first[:, lanes] + wts[1] * second[:, lanes]
        xs[i, my_half, :] += upd[:, lanes]
    last = remote(xs.at[other], xr, sw_s.at[7], sw_r.at[7], partner)
    last.start()
    last.wait_recv()
    out[...] = (xs[c] + xr[...]).astype(BF16)

    for copy in halo + swap_w + [swap_pk, swap_tg, swap_wc, swap_ub, last]:
        copy.wait_send()
    many = pl.ds(0, n_y - 1)
    pltpu.make_async_copy(wc.at[many, own_rows], wc.at[many, own_rows], w_s).wait()
    pltpu.make_async_copy(stats.at[many], stats.at[many], st_s).wait()
    pltpu.make_async_copy(gains.at[many], gains.at[many], gn_s).wait()
    pltpu.make_async_copy(devs.at[many], devs.at[many], a_s).wait()
    pltpu.make_async_copy(gath.at[most], gath.at[most], d_s).wait()
    pltpu.make_async_copy(rows.at[many], rows.at[many], g_s).wait()
    pltpu.make_async_copy(sbuf, sbuf, r_s).wait()
    pltpu.make_async_copy(eo.at[most], eo.at[most], b_s).wait()


def solution(mesh):
    n_sp, n_y = mesh.shape["sp"], mesh.shape["tp"] // 2

    def local(cv, cg, taps, gain, ow, res, ids, rw, eg, eu, ed):
        tok, ch = cv.shape
        width = res.shape[1]
        cols = width // n_y
        ff = eg.shape[2]
        slots = tok * ids.shape[1]
        half = tok // 2
        vm, hbm = pl.BlockSpec(memory_space=pltpu.VMEM), pl.BlockSpec(memory_space=pl.ANY)
        dma = pltpu.SemaphoreType.DMA
        scratch = [
            pltpu.VMEM((HALO + tok, 2 * ch), BF16),
            pltpu.VMEM((HALO + tok, 2 * ch), BF16),
            pltpu.VMEM((40, 2 * ch), F32),
            pltpu.VMEM((40, 2 * ch), F32),
            pltpu.VMEM((HALO + half, 2 * ch), F32),
            pltpu.VMEM((n_y, 8, half), F32),
            pltpu.VMEM((n_y, 8, 2 * ch), F32),
            pltpu.VMEM((n_y, 2 * ch, half), F32),
            pltpu.VMEM((n_y, 2 * ch, half), BF16),
            pltpu.VMEM((n_y, 2 * ch, cols), BF16),
            pltpu.VMEM((half, cols), BF16),
            pltpu.VMEM((half, cols), F32),
            pltpu.VMEM((tok, cols), BF16),
            pltpu.VMEM((2, slots, tok), BF16),
            pltpu.VMEM((2, tok, 128), F32),
            pltpu.VMEM((slots, cols), BF16),
            pltpu.VMEM((n_y, slots, cols), BF16),
            pltpu.VMEM((4, width, ff), BF16),
            pltpu.VMEM((2 * ff, width), BF16),
            pltpu.VMEM((4, slots, ff), F32),
            pltpu.VMEM((slots, 128), F32),
            pltpu.VMEM((slots, 2 * ff), BF16),
            pltpu.VMEM((n_y - 1, slots, cols), BF16),
            pltpu.VMEM((n_y - 1, slots, cols), BF16),
            pltpu.VMEM((slots, cols), BF16),
            pltpu.VMEM((slots, cols), BF16),
            pltpu.VMEM((2, tok, cols // 2), F32),
            pltpu.VMEM((tok, cols // 2), F32),
            dma((6,)), dma((8,)), dma((8,)), dma((2,)), dma((2,)),
            dma, dma((n_y,)), dma, dma((n_y,)), dma, dma((n_y,)), dma, dma((n_y,)),
            dma, dma((n_sp,)), dma, dma((n_y - 1, 8)), dma, dma((n_y - 1, 8)),
            dma, dma,
        ]
        return pl.pallas_call(
            functools.partial(layer, n_sp, n_y),
            out_shape=jax.ShapeDtypeStruct((tok, cols // 2), BF16),
            in_specs=[vm, vm, vm, vm, hbm, hbm, vm, vm, hbm, hbm, hbm],
            out_specs=vm,
            scratch_shapes=scratch,
            compiler_params=pltpu.CompilerParams(
                collective_id=0, has_side_effects=True, vmem_limit_bytes=56 << 20
            ),
        )(cv.T, cg.T, taps, gain.reshape(1, ch), ow, res, ids.T, rw.T, eg, eu, ed)

    placed = (
        P("sp", "tp"), P("sp", "tp"), P(None, "tp"), P("tp"), P("tp", None), P("sp", None),
        P("sp", None), P("sp", None), P("sp", None, "tp"), P("sp", None, "tp"), P("sp", "tp", None),
    )
    return jax.shard_map(local, mesh=mesh, in_specs=placed, out_specs=P("sp", "tp"), check_vma=False)
```

```python
import functools

import jax
import jax.numpy as jnp
from jax import lax
from jax.experimental import pallas as pl
from jax.experimental.pallas import tpu as pltpu
from jax.sharding import PartitionSpec as P

MESH = pl.DeviceIdType.MESH
F32, BF16 = jnp.float32, jnp.bfloat16
HALO = 32
STREAMS = 8
UNITS = 4
ORDER = (0, 7, 1, 6, 2, 5, 3, 4)


def iota(shape, dim):
    return lax.broadcasted_iota(jnp.int32, shape, dim)


def matmul(a, b, precision=None):
    return jnp.dot(a, b, preferred_element_type=F32, precision=precision)


def matmul_t(a, b):
    return lax.dot_general(a, b, (((0,), (0,)), ((), ())), preferred_element_type=F32)


def layer(
    n_sp, n_y,
    cv, cg, taps, gain, ow, res, ids, rw, eg, eu, ed,
    out,
    pk_own, pk_par, tg_own, tg_par, gext, stats, gains, gcol, devs, wc, resv, upd, ub, gs, wts,
    gath, rows, wgu, wd, acc, ssq, hid, sbuf, rbuf, eo, back, xs, xr,
    l_sem, sw_s, sw_r, h_s, h_r, w_s, w_r, st_s, st_r, a_s, a_r, gn_s, gn_r, d_s, d_r, g_s, g_r,
    r_s, r_r, b_s, b_r,
):
    sp, tp = lax.axis_index("sp"), lax.axis_index("tp")
    y, c = tp // 2, tp % 2
    other = 1 - c
    n_x = n_sp // STREAMS
    z, x = sp // n_x, sp % n_x
    partner = (sp, y * 2 + other)
    ch, tok = cv.shape
    half = tok // 2
    wide = 2 * ch
    width = res.shape[1]
    cols = width // n_y
    ff = eg.shape[2]
    slots = gath.shape[0]
    per = slots // n_sp
    size = slots // UNITS
    far = n_y // 2

    def column(k):
        return (sp, lax.rem(y + k, n_y) * 2 + c)

    def remote(src, dst, s, r, dev):
        return pltpu.make_async_remote_copy(
            src_ref=src, dst_ref=dst, send_sem=s, recv_sem=r, device_id=dev, device_id_type=MESH
        )

    my_cols = pl.ds(pl.multiple_of(y * cols, cols), cols)
    my_half = pl.ds(pl.multiple_of(c * half, half), half)
    own_rows = pl.ds(pl.multiple_of(c * ch, ch), ch)
    loads = [
        pltpu.make_async_copy(res.at[my_half, my_cols], resv, l_sem.at[0]),
        pltpu.make_async_copy(eg.at[0], wgu.at[0], l_sem.at[1]),
        pltpu.make_async_copy(eu.at[0], wgu.at[2], l_sem.at[2]),
        pltpu.make_async_copy(ed.at[0], wd.at[pl.ds(0, ff)], l_sem.at[3]),
        pltpu.make_async_copy(ow.at[:, my_cols], wc.at[y, own_rows], l_sem.at[4]),
    ]
    for load in loads:
        load.start()

    barrier = pltpu.get_barrier_semaphore()

    def greet(dev):
        pl.semaphore_signal(barrier, inc=1, device_id=dev, device_id_type=MESH)

    nxt = lax.rem(sp + 1, n_sp)
    prv = lax.rem(sp + n_sp - 1, n_sp)

    @pl.loop(1, n_sp)
    def _(k):
        greet((lax.rem(sp + k, n_sp), tp))

    @pl.loop(1, n_y)
    def _(k):
        greet(column(k))

    greet((nxt, y * 2 + other))
    greet((prv, y * 2 + other))
    greet(partner)

    lane = iota((ch, wide), 1)
    chan = iota((ch, wide), 0)
    put_low = (lane == chan).astype(BF16)
    put_high = (lane == chan + ch).astype(BF16)
    pk_own[pl.ds(HALO, tok), :] = (
        matmul_t(cv[...], put_low) + matmul_t(cg[...], put_high)
    ).astype(BF16)
    n_taps = taps.shape[0]
    tg_own[...] = jnp.zeros_like(tg_own)
    tg_own[pl.ds(0, n_taps), :] = matmul(taps[...], put_low)
    tg_own[pl.ds(n_taps, 1), :] = matmul(
        jnp.broadcast_to(gain[...], (8, ch)), put_low.astype(F32), lax.Precision.HIGHEST
    )[0:1]

    expert = iota((128, tok), 0)
    id0, id1 = ids[0:1, :], ids[1:2, :]
    hot0, hot1 = (id0 == expert).astype(F32), (id1 == expert).astype(F32)
    before = (iota((tok, tok), 0) < iota((tok, tok), 1)).astype(BF16)
    earlier = matmul((hot0 + hot1).astype(BF16), before)
    place = iota((slots, tok), 0)
    for k, (ident, hot) in enumerate(((id0, hot0), (id1, hot1))):
        rank = jnp.sum(earlier * hot, axis=0, keepdims=True).astype(jnp.int32) - c * per
        slot = jnp.where((rank >= 0) & (rank < per), ident * per + rank, -1)
        gs[k] = jnp.where(place == slot, 1.0, 0.0).astype(BF16)
        wts[k] = jnp.transpose(jnp.broadcast_to(rw[k : k + 1, :], (128, tok)))

    pl.semaphore_wait(barrier, 3 + (n_y - 1) + (n_sp - 1))

    body = pl.ds(HALO, tok)
    head = pl.ds(0, HALO)
    tail = pl.ds(tok, HALO)
    halo = [
        remote(pk_own.at[tail], pk_own.at[head], h_s.at[0], h_r.at[0], (nxt, tp)),
        remote(pk_own.at[tail], pk_par.at[head], h_s.at[1], h_r.at[1], (nxt, y * 2 + other)),
    ]
    for copy in halo:
        copy.start()
    swap_tg = remote(tg_own, tg_par, sw_s.at[1], sw_r.at[1], partner)
    swap_pk = remote(pk_own.at[body], pk_par.at[body], sw_s.at[0], sw_r.at[0], partner)
    swap_tg.start()
    swap_pk.start()

    @pl.loop(1, n_y)
    def _(k):
        dst_chip = lax.rem(y + k, n_y)
        far_cols = pl.ds(pl.multiple_of(dst_chip * cols, cols), cols)
        remote(ow.at[:, far_cols], wc.at[y, own_rows], w_s, w_r.at[y], column(k)).start()

    swap_w = [
        remote(eg.at[0], wgu.at[1], sw_s.at[2], sw_r.at[2], partner),
        remote(eu.at[0], wgu.at[3], sw_s.at[3], sw_r.at[3], partner),
        remote(ed.at[0], wd.at[pl.ds(ff, ff)], sw_s.at[4], sw_r.at[4], partner),
    ]
    for copy in swap_w:
        copy.start()

    lane2, chan2 = iota((wide, wide), 1), iota((wide, wide), 0)

    def pick(first, to):
        return (
            (chan2 >= first) & (chan2 < first + ch) & (lane2 == chan2 - first + to * ch)
        ).astype(BF16)

    swap_tg.wait_recv()
    tg = matmul(tg_own[...], pick(0, c).astype(F32), lax.Precision.HIGHEST) + matmul(
        tg_par[...], pick(0, other).astype(F32), lax.Precision.HIGHEST
    )

    def everywhere(buf, s, r):
        @pl.loop(1, n_y)
        def _(k):
            remote(buf.at[y], buf.at[y], s, r.at[y], column(k)).start()

    def arrived(buf, s, r, k):
        origin = lax.rem(y + k, n_y)
        remote(buf.at[origin], buf.at[origin], s, r.at[origin], column(k)).wait_recv()
        return origin

    swap_pk.wait_recv()
    for copy in halo:
        copy.wait_recv()
    span = pl.ds(pl.multiple_of(c * half, half), half + HALO)
    mine, theirs = pk_own[span, :], pk_par[span, :]
    value = matmul(mine, pick(0, c)) + matmul(theirs, pick(0, other))
    gate = matmul(mine, pick(ch, c)) + matmul(theirs, pick(ch, other))
    gated = value / (1.0 + jnp.exp(-gate))
    start = (iota(gated.shape, 0) < HALO) & (sp == 0) & (c == 0)
    gext[...] = jnp.where(start, 0.0, gated)
    filtered = jnp.zeros((half, wide), F32)
    for i in range(n_taps):
        filtered = filtered + tg[i : i + 1, :] * gext[pl.ds(i + HALO + 1 - n_taps, half), :]

    turned = jnp.transpose(filtered)
    mean = jnp.sum(turned, axis=0, keepdims=True) / wide
    turned = turned - mean
    spread = jnp.sum(turned * turned, axis=0, keepdims=True) / wide
    devs[y] = turned.astype(BF16)
    stats[y] = jnp.where(iota((8, half), 0) == 0, mean, spread)
    gains[y] = jnp.broadcast_to(tg[n_taps : n_taps + 1, :], (8, wide))
    everywhere(stats, st_s, st_r)
    everywhere(gains, gn_s, gn_r)
    everywhere(devs, a_s, a_r)

    loads[4].wait()

    @pl.loop(1, n_y)
    def _(k):
        origin = lax.rem(y + k, n_y)
        remote(
            wc.at[origin, own_rows], wc.at[origin, own_rows], w_s, w_r.at[origin], column(k)
        ).wait_recv()

    swap_wc = remote(wc.at[:, own_rows], wc.at[:, own_rows], sw_s.at[5], sw_r.at[5], partner)
    swap_wc.start()

    @pl.loop(1, n_y)
    def _(k):
        arrived(stats, st_s, st_r, k)
        arrived(gains, gn_s, gn_r, k)

    average = stats[0, 0:1, :]
    for o in range(1, n_y):
        average = average + stats[o, 0:1, :]
    average = average / n_y
    variance = jnp.zeros_like(average)
    for o in range(n_y):
        gap = stats[o, 0:1, :] - average
        variance = variance + (stats[o, 1:2, :] + gap * gap)
    scale = lax.rsqrt(variance / n_y + 1e-05)
    for o in range(n_y):
        gcol[o] = jnp.transpose(jnp.broadcast_to(gains[o, 0:1, :], (half, wide))) * scale

    def mixed(origin):
        shift = stats[origin, 0:1, :] - average
        normed = (devs[origin].astype(F32) + shift) * gcol[origin]
        activated = (normed / (1.0 + jnp.exp(-normed))).astype(BF16)
        return matmul_t(activated, wc[origin])

    loads[0].wait()
    swap_wc.wait_recv()
    upd[...] = resv[...].astype(F32) + mixed(y)
    for k in (1, 7, 2, 6, 3, 5, 4) if n_y == 8 else range(1, n_y):
        upd[...] += mixed(arrived(devs, a_s, a_r, k))

    ub[my_half, :] = upd[...].astype(BF16)
    swap_ub = remote(ub.at[my_half], ub.at[my_half], sw_s.at[6], sw_r.at[6], partner)
    swap_ub.start()
    swap_ub.wait_recv()

    gath[...] = matmul(gs[0] + gs[1], ub[...]).astype(BF16)

    def at(k):
        return pl.ds(pl.multiple_of(k * per, per), per)

    def below(j):
        return lax.rem(z + STREAMS - j, STREAMS)

    def above(j):
        return lax.rem(z + j, STREAMS)

    for place_j, j in enumerate(ORDER):
        spot = place_j * n_x + x
        for i in range(n_x):
            dst = below(j) * n_x + lax.rem(x + i, n_x)
            if i == 0 and j == 0:
                keep = pltpu.make_async_copy(gath.at[at(dst)], rows.at[y, at(spot)], d_r.at[spot])
                keep.start()
            else:
                remote(gath.at[at(dst)], rows.at[y, at(spot)], d_s, d_r.at[spot], (dst, tp)).start()

    for load in loads[1:4]:
        load.wait()
    for copy in swap_w:
        copy.wait_recv()
    acc[...] = jnp.zeros_like(acc)
    ssq[...] = jnp.zeros_like(ssq)

    def unit(u):
        return pl.ds(u * size, size)

    def piece(u, d):
        return pl.ds(u * size + d * (size // 2), size // 2)

    def chip(k):
        return lax.rem(y + n_y + k, n_y)

    def hop(h, d, u):
        origin = chip(1 - h if d == 0 else h - 1)
        block = rows.at[origin, unit(u) if h < far else piece(u, d)]
        return remote(block, block, g_s, g_r.at[d, h - 1, u], column(1 if d == 0 else n_y - 1))

    def hop_in(h, d, u):
        origin = chip(-h if d == 0 else h)
        block = rows.at[origin, unit(u) if h < far else piece(u, d)]
        return remote(block, block, g_s, g_r.at[d, h - 1, u], partner)

    def deep(origin):
        return pl.ds(pl.multiple_of(origin * cols, cols), cols)

    def folded(v):
        v = v.astype(F32)
        v = v * v
        total = v[:, 0:128]
        for i in range(1, cols // 128):
            total = total + v[:, i * 128 : (i + 1) * 128]
        return total

    def accumulate(origin, block):
        v = rows[origin, block, :]
        ssq[block, :] += folded(v)
        for i in range(4):
            acc[i, block, :] += matmul(v, wgu[i, deep(origin), :])

    def finish(u):
        block = unit(u)
        for origin in (chip(1 - far), chip(far - 1), chip(far)):
            accumulate(origin, block)
        rms = lax.rsqrt(jnp.sum(ssq[block, :], axis=1, keepdims=True) / width + 1e-06)
        for i in range(2):
            g = acc[i, block, :] * rms
            v = acc[2 + i, block, :] * rms
            hid[block, i * ff : (i + 1) * ff] = (g / (1.0 + jnp.exp(-g)) * v).astype(BF16)

    def product(u, chunk):
        return matmul(hid[unit(u), :], wd[:, deep(chunk)])

    def sum_copy(r, d, u):
        block = unit(u) if r > 0 else piece(u, d)
        return remote(
            sbuf.at[d, r, block], rbuf.at[d, r, block], r_s, r_r.at[d, r, u],
            column(1 if d == 0 else n_y - 1),
        )

    def first_sums(u):
        partial = product(u, chip(far)).astype(BF16)
        for d in range(2):
            sbuf[d, 0, piece(u, d), :] = partial[d * (size // 2) : (d + 1) * (size // 2)]
            sum_copy(0, d, u).start()

    def next_sums(r, u):
        for d in range(2):
            partial = product(u, chip(far - r if d == 0 else r - far))
            sum_copy(r - 1, d, u).wait_recv()
            if r == 1:
                here, there = (piece(u, 0), piece(u, 1)) if d == 0 else (piece(u, 1), piece(u, 0))
                parts = (partial[0 : size // 2], partial[size // 2 :])
                sbuf[d, r, here, :] = (parts[d] + rbuf[d, 0, here, :].astype(F32)).astype(BF16)
                sbuf[d, r, there, :] = parts[1 - d].astype(BF16)
            else:
                partial = partial + rbuf[d, r - 1, unit(u), :].astype(F32)
                sbuf[d, r, unit(u), :] = partial.astype(BF16)
            sum_copy(r, d, u).start()

    def send_back(u):
        partial = product(u, y)
        for d in range(2):
            sum_copy(far - 1, d, u).wait_recv()
            partial = partial + rbuf[d, far - 1, unit(u), :].astype(F32)
        eo[unit(u), :] = partial.astype(BF16)
        for place_j in range(2 * u, 2 * u + 2):
            for i in range(n_x):
                spot = place_j * n_x + i
                dst = above(ORDER[place_j]) * n_x + i
                if place_j == 0:

                    @pl.when(x != i)
                    def _():
                        remote(eo.at[at(spot)], back.at[at(sp)], b_s, b_r, (dst, tp)).start()

                else:
                    remote(eo.at[at(spot)], back.at[at(sp)], b_s, b_r, (dst, tp)).start()

    everything = pl.ds(0, slots)
    for u in range(UNITS):
        for k in range(2 * u * n_x, 2 * (u + 1) * n_x):
            spot = rows.at[y, at(k)]
            pltpu.make_async_copy(spot, spot, d_r.at[k]).wait()
        for d in range(2):
            hop(1, d, u).start()
    accumulate(y, everything)

    def pass_on(h, u):
        for d in range(2):
            hop_in(h, d, u).wait_recv()
            hop(h + 1, d, u).start()

    def through(u):
        for d in range(2):
            hop_in(far, d, u).wait_recv()
        finish(u)
        first_sums(u)

    for h in range(1, far - 1):
        for u in range(UNITS):
            pass_on(h, u)
        accumulate(chip(-h), everything)
        accumulate(chip(h), everything)
    behind = 3
    for u in range(UNITS + behind):
        if u < UNITS:
            pass_on(far - 1, u)
        if u >= behind:
            through(u - behind)

    for r in range(1, far):
        for u in range(UNITS):
            next_sums(r, u)
    for u in range(UNITS):
        send_back(u)

    stay = pltpu.make_async_copy(eo.at[at(x)], back.at[at(sp)], l_sem.at[5])
    stay.start()
    stay.wait()
    most = pl.ds(0, slots - per)
    pltpu.make_async_copy(back.at[most], back.at[most], b_r).wait()

    first, second = matmul_t(gs[0], back[...]), matmul_t(gs[1], back[...])
    for i in range(2):
        lanes = slice(i * (cols // 2), (i + 1) * (cols // 2))
        xs[i] = wts[0] * first[:, lanes] + wts[1] * second[:, lanes]
        xs[i, my_half, :] += upd[:, lanes]
    last = remote(xs.at[other], xr, sw_s.at[7], sw_r.at[7], partner)
    last.start()
    last.wait_recv()
    out[...] = (xs[c] + xr[...]).astype(BF16)

    for copy in halo + swap_w + [swap_pk, swap_tg, swap_wc, swap_ub, last]:
        copy.wait_send()
    many = pl.ds(0, n_y - 1)
    pltpu.make_async_copy(wc.at[many, own_rows], wc.at[many, own_rows], w_s).wait()
    pltpu.make_async_copy(stats.at[many], stats.at[many], st_s).wait()
    pltpu.make_async_copy(gains.at[many], gains.at[many], gn_s).wait()
    pltpu.make_async_copy(devs.at[many], devs.at[many], a_s).wait()
    pltpu.make_async_copy(gath.at[most], gath.at[most], d_s).wait()
    pltpu.make_async_copy(rows.at[many], rows.at[many], g_s).wait()
    pltpu.make_async_copy(rows.at[many], rows.at[many], r_s).wait()
    pltpu.make_async_copy(eo.at[most], eo.at[most], b_s).wait()


def solution(mesh):
    n_sp, n_y = mesh.shape["sp"], mesh.shape["tp"] // 2

    def local(cv, cg, taps, gain, ow, res, ids, rw, eg, eu, ed):
        tok, ch = cv.shape
        width = res.shape[1]
        cols = width // n_y
        ff = eg.shape[2]
        slots = tok * ids.shape[1]
        half = tok // 2
        vm, hbm = pl.BlockSpec(memory_space=pltpu.VMEM), pl.BlockSpec(memory_space=pl.ANY)
        dma = pltpu.SemaphoreType.DMA
        scratch = [
            pltpu.VMEM((HALO + tok, 2 * ch), BF16),
            pltpu.VMEM((HALO + tok, 2 * ch), BF16),
            pltpu.VMEM((40, 2 * ch), F32),
            pltpu.VMEM((40, 2 * ch), F32),
            pltpu.VMEM((HALO + half, 2 * ch), F32),
            pltpu.VMEM((n_y, 8, half), F32),
            pltpu.VMEM((n_y, 8, 2 * ch), F32),
            pltpu.VMEM((n_y, 2 * ch, half), F32),
            pltpu.VMEM((n_y, 2 * ch, half), BF16),
            pltpu.VMEM((n_y, 2 * ch, cols), BF16),
            pltpu.VMEM((half, cols), BF16),
            pltpu.VMEM((half, cols), F32),
            pltpu.VMEM((tok, cols), BF16),
            pltpu.VMEM((2, slots, tok), BF16),
            pltpu.VMEM((2, tok, 128), F32),
            pltpu.VMEM((slots, cols), BF16),
            pltpu.VMEM((n_y, slots, cols), BF16),
            pltpu.VMEM((4, width, ff), BF16),
            pltpu.VMEM((2 * ff, width), BF16),
            pltpu.VMEM((4, slots, ff), F32),
            pltpu.VMEM((slots, 128), F32),
            pltpu.VMEM((slots, 2 * ff), BF16),
            pltpu.VMEM((2, n_y // 2, slots, cols), BF16),
            pltpu.VMEM((2, n_y // 2, slots, cols), BF16),
            pltpu.VMEM((slots, cols), BF16),
            pltpu.VMEM((slots, cols), BF16),
            pltpu.VMEM((2, tok, cols // 2), F32),
            pltpu.VMEM((tok, cols // 2), F32),
            dma((6,)), dma((8,)), dma((8,)), dma((2,)), dma((2,)),
            dma, dma((n_y,)), dma, dma((n_y,)), dma, dma((n_y,)), dma, dma((n_y,)),
            dma, dma((n_sp,)), dma, dma((2, n_y // 2, UNITS)), dma, dma((2, n_y // 2, UNITS)),
            dma, dma,
        ]
        return pl.pallas_call(
            functools.partial(layer, n_sp, n_y),
            out_shape=jax.ShapeDtypeStruct((tok, cols // 2), BF16),
            in_specs=[vm, vm, vm, vm, hbm, hbm, vm, vm, hbm, hbm, hbm],
            out_specs=vm,
            scratch_shapes=scratch,
            compiler_params=pltpu.CompilerParams(
                collective_id=0, has_side_effects=True, vmem_limit_bytes=56 << 20
            ),
        )(cv.T, cg.T, taps, gain.reshape(1, ch), ow, res, ids.T, rw.T, eg, eu, ed)

    placed = (
        P("sp", "tp"), P("sp", "tp"), P(None, "tp"), P("tp"), P("tp", None), P("sp", None),
        P("sp", None), P("sp", None), P("sp", None, "tp"), P("sp", None, "tp"), P("sp", "tp", None),
    )
    return jax.shard_map(local, mesh=mesh, in_specs=placed, out_specs=P("sp", "tp"), check_vma=False)
```

```python
import functools

import jax
import jax.numpy as jnp
from jax import lax
from jax.experimental import pallas as pl
from jax.experimental.pallas import tpu as pltpu
from jax.sharding import PartitionSpec as P

MESH = pl.DeviceIdType.MESH
F32, BF16 = jnp.float32, jnp.bfloat16
HALO = 32
STREAMS = 8
UNITS = 4
ORDER = (0, 7, 1, 6, 2, 5, 3, 4)


def iota(shape, dim):
    return lax.broadcasted_iota(jnp.int32, shape, dim)


def matmul(a, b, precision=None):
    return jnp.dot(a, b, preferred_element_type=F32, precision=precision)


def matmul_t(a, b):
    return lax.dot_general(a, b, (((0,), (0,)), ((), ())), preferred_element_type=F32)


def layer(
    n_sp, n_y,
    cv_in, cg_in, taps_in, gain_in, ow, res, ids_in, rw_in, eg, eu, ed,
    out,
    cv, cg, taps, gain, ids, rw, pk_own, pk_par, tg_own, tg_par, gext, stats, gcol, devs, wc, resv, upd, updx, ups, ub, gs, takes, wts,
    first_rows, gath, rows, wgu, wd, acc, ssq, hid, sbuf, rbuf, eo, back,
    l_sem, sw_s, sw_r, h_s, h_r, w_s, w_r, st_s, st_r, a_s, a_r, x_s, x_r, c_s, c_r, d_s, d_r, g_s, g_r,
    r_s, r_r, b_s, b_r, tok_sem,
):
    sp, tp = lax.axis_index("sp"), lax.axis_index("tp")
    y, c = tp // 2, tp % 2
    other = 1 - c
    n_x = n_sp // STREAMS
    z, x = sp // n_x, sp % n_x
    partner = (sp, y * 2 + other)
    ch, tok = cv.shape
    half = tok // 2
    wide = 2 * ch
    width = res.shape[1]
    cols = width // n_y
    ff = eg.shape[2]
    slots = gath.shape[0]
    per = slots // n_sp
    size = slots // UNITS
    far = n_y // 2

    def column(k):
        return (sp, lax.rem(y + k, n_y) * 2 + c)

    def chip(k):
        return lax.rem(y + n_y + k, n_y)

    def remote(src, dst, s, r, dev):
        return pltpu.make_async_remote_copy(
            src_ref=src, dst_ref=dst, send_sem=s, recv_sem=r, device_id=dev, device_id_type=MESH
        )

    barrier = pltpu.get_barrier_semaphore()

    def greet(dev):
        pl.semaphore_signal(barrier, inc=1, device_id=dev, device_id_type=MESH)

    nxt = lax.rem(sp + 1, n_sp)
    prv = lax.rem(sp + n_sp - 1, n_sp)
    z_next = (lax.rem(z + 1, STREAMS) * n_x + x, tp)
    z_prev = (lax.rem(z + STREAMS - 1, STREAMS) * n_x + x, tp)
    near = [column(k) for k in range(n_y - 1, 0, -1)]
    for i in range(1, n_x):
        side = z * n_x + lax.rem(x + i, n_x)
        near += [(side, tp), (side, y * 2 + other)]
    near += [z_next, z_prev, partner]
    for dev in near:
        greet(dev)

    @pl.when(sp < n_sp - 1)
    def _():
        greet((nxt, tp))
        greet((nxt, y * 2 + other))

    @pl.when(sp > 0)
    def _():
        greet((prv, tp))
        greet((prv, y * 2 + other))

    ends = jnp.where(sp > 0, 2, 0) + jnp.where(sp < n_sp - 1, 2, 0)

    def token(r):
        for dev in (z_next, z_prev):
            pl.semaphore_signal(tok_sem.at[r], inc=1, device_id=dev, device_id_type=MESH)

    my_cols = pl.ds(pl.multiple_of(y * cols, cols), cols)
    my_half = pl.ds(pl.multiple_of(c * half, half), half)
    own_rows = pl.ds(pl.multiple_of(c * ch, ch), ch)
    half_ch = ch // 2
    pair_x = sp + 1 - 2 * (x % 2)
    pair_rows = pl.ds(pl.multiple_of((x % 2) * half_ch, half_ch), half_ch)
    own_pair = pl.ds(pl.multiple_of(c * ch + (x % 2) * half_ch, half_ch), half_ch)
    small = [
        pltpu.make_async_copy(src, dst, l_sem.at[6 + i])
        for i, (src, dst) in enumerate(
            ((cv_in, cv), (cg_in, cg), (taps_in, taps), (gain_in, gain), (ids_in, ids), (rw_in, rw))
        )
    ]
    loads = [
        pltpu.make_async_copy(res.at[my_half, my_cols], resv, l_sem.at[0]),
        pltpu.make_async_copy(eg.at[0], wgu.at[0], l_sem.at[1]),
        pltpu.make_async_copy(eu.at[0], wgu.at[2], l_sem.at[2]),
        pltpu.make_async_copy(ed.at[0], wd.at[pl.ds(0, ff)], l_sem.at[3]),
        pltpu.make_async_copy(ow.at[pair_rows, my_cols], wc.at[y, own_pair], l_sem.at[4]),
    ]
    for load in small + loads:
        load.start()

    lane = iota((ch, wide), 1)
    chan = iota((ch, wide), 0)
    put_low = (lane == chan).astype(BF16)
    put_high = (lane == chan + ch).astype(BF16)
    for load in small[0:4]:
        load.wait()
    pk_own[pl.ds(HALO, tok), :] = (
        matmul_t(cv[...], put_low) + matmul_t(cg[...], put_high)
    ).astype(BF16)
    n_taps = taps.shape[0]
    tg_own[...] = jnp.zeros_like(tg_own)
    tg_own[pl.ds(0, n_taps), :] = matmul(taps[...], put_low)
    tg_own[pl.ds(n_taps, 1), :] = matmul(
        jnp.broadcast_to(gain[...], (8, ch)), put_low.astype(F32), lax.Precision.HIGHEST
    )[0:1]

    pl.semaphore_wait(barrier, len(near) + ends)

    body = pl.ds(HALO, tok)
    head = pl.ds(0, HALO)
    tail = pl.ds(tok, HALO)
    halo = [
        remote(pk_own.at[tail], pk_own.at[head], h_s.at[0], h_r.at[0], (nxt, tp)),
        remote(pk_own.at[tail], pk_par.at[head], h_s.at[1], h_r.at[1], (nxt, y * 2 + other)),
    ]

    @pl.when(sp < n_sp - 1)
    def _():
        for copy in halo:
            copy.start()

    @pl.when(sp == 0)
    def _():
        pk_own[head, :] = jnp.zeros((HALO, wide), BF16)
        pk_par[head, :] = jnp.zeros((HALO, wide), BF16)

    swap_tg = remote(tg_own, tg_par, sw_s.at[1], sw_r.at[1], partner)
    swap_pk = remote(pk_own.at[body], pk_par.at[body], sw_s.at[0], sw_r.at[0], partner)
    swap_tg.start()
    swap_pk.start()

    outward = (1, n_y - 1, 2, n_y - 2, 3, n_y - 3, far)
    for k in outward:
        far_cols = pl.ds(pl.multiple_of(chip(k) * cols, cols), cols)
        remote(ow.at[pair_rows, far_cols], wc.at[y, own_pair], w_s, w_r.at[y], column(k)).start()

    token(0)
    swap_w = [
        remote(eg.at[0], wgu.at[1], sw_s.at[2], sw_r.at[2], partner),
        remote(eu.at[0], wgu.at[3], sw_s.at[3], sw_r.at[3], partner),
        remote(ed.at[0], wd.at[pl.ds(ff, ff)], sw_s.at[4], sw_r.at[4], partner),
    ]
    for load in small[4:6]:
        load.wait()
    expert = iota((128, tok), 0)
    id0, id1 = ids[0:1, :], ids[1:2, :]
    hot0, hot1 = (id0 == expert).astype(F32), (id1 == expert).astype(F32)
    before = (iota((tok, tok), 0) < iota((tok, tok), 1)).astype(BF16)
    earlier = matmul((hot0 + hot1).astype(BF16), before)
    place = iota((slots, tok), 0) + c * slots
    slot_rows = []
    for ident, hot in ((id0, hot0), (id1, hot1)):
        rank = jnp.sum(earlier * hot, axis=0, keepdims=True).astype(jnp.int32)
        slot_rows.append(jnp.where(rank < per, 0, slots - per) + ident * per + rank)
    gs[...] = jnp.where((place == slot_rows[0]) | (place == slot_rows[1]), 1.0, 0.0).astype(BF16)

    lane2, chan2 = iota((wide, wide), 1), iota((wide, wide), 0)

    def pick(first, to):
        return (
            (chan2 >= first) & (chan2 < first + ch) & (lane2 == chan2 - first + to * ch)
        ).astype(BF16)

    swap_tg.wait_recv()
    tg = matmul(tg_own[...], pick(0, c).astype(F32), lax.Precision.HIGHEST) + matmul(
        tg_par[...], pick(0, other).astype(F32), lax.Precision.HIGHEST
    )

    def everywhere(buf, s, r):
        @pl.loop(1, n_y)
        def _(k):
            remote(buf.at[y], buf.at[y], s, r.at[y], column(k)).start()

    def arrived(buf, s, r, k):
        origin = lax.rem(y + k, n_y)
        remote(buf.at[origin], buf.at[origin], s, r.at[origin], column(k)).wait_recv()
        return origin

    def tokens(r):
        pl.semaphore_wait(tok_sem.at[r], 2)
        if r < STREAMS // 2 - 1:
            token(r + 1)

    tokens(0)
    swap_pk.wait_recv()

    @pl.when(sp > 0)
    def _():
        for copy in halo:
            copy.wait_recv()

    span = pl.ds(pl.multiple_of(c * half, half), half + HALO)
    mine, theirs = pk_own[span, :], pk_par[span, :]
    value = matmul(mine, pick(0, c)) + matmul(theirs, pick(0, other))
    gate = matmul(mine, pick(ch, c)) + matmul(theirs, pick(ch, other))
    gated = value / (1.0 + jnp.exp(-gate))
    start = (iota(gated.shape, 0) < HALO) & (sp == 0) & (c == 0)
    gext[...] = jnp.where(start, 0.0, gated)
    filtered = jnp.zeros((half, wide), F32)
    for i in range(n_taps):
        filtered = filtered + tg[i : i + 1, :] * gext[pl.ds(i + HALO + 1 - n_taps, half), :]

    turned = jnp.transpose(filtered)
    mean = jnp.sum(turned, axis=0, keepdims=True) / wide
    turned = turned - mean
    spread = jnp.sum(turned * turned, axis=0, keepdims=True) / wide
    devs[y] = turned.astype(BF16)
    line = iota((8, half), 0)
    note = jnp.where(line == 1, spread, jnp.broadcast_to(tg[n_taps : n_taps + 1, :], (8, half)))
    stats[y] = jnp.where(line == 0, mean, note)
    everywhere(stats, st_s, st_r)

    def tell(origin, k, r):
        remote(devs.at[origin], devs.at[origin], a_s, r, column(k)).start()

    for k in (2, n_y - 2, 1, n_y - 1):
        tell(y, k, a_r.at[y])
    tokens(1)

    def hear(k):
        origin = lax.rem(y + k, n_y)
        remote(devs.at[origin], devs.at[origin], a_s, a_r.at[origin], partner).wait_recv()
        return origin

    def share(k):
        block = wc.at[chip(k), own_pair]
        if k == 0:
            loads[4].wait()
        else:
            remote(block, block, w_s, w_r.at[chip(k)], partner).wait_recv()
        remote(block, block, x_s, x_r.at[chip(k)], (pair_x, tp)).start()

    for k in (0,) + outward[0:4]:
        share(k)
    for k, on in ((n_y - 2, 1), (2, n_y - 1)):
        origin = hear(k)
        tell(origin, on, a_r.at[origin])
        piece_of = devs.at[origin, pl.ds(0 if on == 1 else ch, ch)]
        sem = a_r.at[origin] if on == 1 else a_r.at[n_y]
        remote(piece_of, piece_of, a_s, sem, column(2 if on == 1 else n_y - 2)).start()
    for k in outward[4:]:
        share(k)
    tokens(2)

    @pl.loop(1, n_y)
    def _(k):
        arrived(stats, st_s, st_r, k)

    average = stats[0, 0:1, :]
    for o in range(1, n_y):
        average = average + stats[o, 0:1, :]
    average = average / n_y
    variance = jnp.zeros_like(average)
    for o in range(n_y):
        gap = stats[o, 0:1, :] - average
        variance = variance + (stats[o, 1:2, :] + gap * gap)
    scale = lax.rsqrt(variance / n_y + 1e-05)
    for o in range(n_y):
        gcol[o] = jnp.transpose(jnp.broadcast_to(stats[o, 2:3, :], (half, wide))) * scale

    def mixed(origin):
        shift = stats[origin, 0:1, :] - average
        normed = (devs[origin].astype(F32) + shift) * gcol[origin]
        activated = (normed / (1.0 + jnp.exp(-normed))).astype(BF16)
        return matmul_t(activated, wc[origin])

    for k in (0,) + outward:
        block = wc.at[chip(k), own_pair]
        remote(block, block, x_s, x_r.at[chip(k)], partner).wait_recv()
        block = wc.at[chip(k), own_rows]
        remote(block, block, c_s, c_r.at[chip(k)], partner).start()

    def whole(k):
        block = wc.at[chip(k), own_rows]
        remote(block, block, c_s, c_r.at[chip(k)], partner).wait_recv()
        return chip(k)

    loads[0].wait()
    whole(0)
    upd[...] = resv[...].astype(F32) + mixed(y)
    for k in outward[0:6]:
        if k not in (2, n_y - 2):
            hear(k)
        upd[...] += mixed(whole(k))
    last_half = devs.at[chip(far), pl.ds(0, ch)]
    for sem in (a_r.at[chip(far)], a_r.at[n_y]):
        remote(last_half, last_half, a_s, sem, partner).wait_recv()
    upd[...] += mixed(whole(far))

    ub[my_half, :] = upd[...].astype(BF16)
    swap_ub = remote(ub.at[my_half], ub.at[my_half], sw_s.at[6], sw_r.at[6], partner)
    swap_ub.start()
    narrow = cols // 2
    for t in range(2):

        @pl.when(c == t)
        def _():
            updx[t] = upd[:, t * narrow : (t + 1) * narrow]
            ups[...] = upd[:, (1 - t) * narrow : (2 - t) * narrow]

    swap_upd = remote(ups, updx.at[c], sw_s.at[7], sw_r.at[7], partner)
    swap_upd.start()
    for copy in swap_w:
        copy.start()
    swap_ub.wait_recv()

    tokens(3)

    def at(k):
        return pl.ds(pl.multiple_of(k * per, per), per)

    def below(j):
        return lax.rem(z + STREAMS - j, STREAMS)

    def above(j):
        return lax.rem(z + j, STREAMS)

    block_z = n_x * per
    for place_j, j in enumerate(ORDER):
        spot = place_j * n_x + x
        to_z = pl.ds(pl.multiple_of(below(j) * block_z, block_z), block_z)
        if place_j < 2:
            picked = matmul(gs[to_z, :], ub[...]).astype(BF16)
            first_rows[pl.ds(place_j * block_z, block_z), :] = picked
        elif place_j == 2:
            gath[...] = matmul(gs[...], ub[...]).astype(BF16)
        for i in range(n_x):
            dst = below(j) * n_x + lax.rem(x + i, n_x)
            if place_j < 2:
                start_at = place_j * block_z + lax.rem(x + i, n_x) * per
                src = first_rows.at[pl.ds(pl.multiple_of(start_at, per), per)]
            else:
                src = gath.at[at(dst)]
            if i == 0 and j == 0:
                keep = pltpu.make_async_copy(src, rows.at[y, at(spot)], d_r.at[spot])
                keep.start()
            else:
                remote(src, rows.at[y, at(spot)], d_s, d_r.at[spot], (dst, tp)).start()

    for k in range(2):
        wts[k] = jnp.transpose(jnp.broadcast_to(rw[k : k + 1, :], (128, tok)))
        slot = jnp.transpose(jnp.broadcast_to(slot_rows[k].astype(F32), (128, tok)))
        for m in range(2 * slots // 128):
            here = (iota((tok, 128), 1) + m * 128).astype(F32)
            takes[k, :, m * 128 : (m + 1) * 128] = jnp.where(slot == here, 1.0, 0.0).astype(BF16)

    acc[...] = jnp.zeros_like(acc)
    ssq[...] = jnp.zeros_like(ssq)

    def unit(u):
        return pl.ds(u * size, size)

    def piece(u, d):
        return pl.ds(u * size + d * (size // 2), size // 2)

    def hop(h, d, u):
        origin = chip(1 - h if d == 0 else h - 1)
        block = rows.at[origin, unit(u) if h < far else piece(u, d)]
        return remote(block, block, g_s, g_r.at[d, h - 1, u], column(1 if d == 0 else n_y - 1))

    def hop_in(h, d, u):
        origin = chip(-h if d == 0 else h)
        block = rows.at[origin, unit(u) if h < far else piece(u, d)]
        return remote(block, block, g_s, g_r.at[d, h - 1, u], partner)

    def deep(origin):
        return pl.ds(pl.multiple_of(origin * cols, cols), cols)

    def folded(v):
        v = v.astype(F32)
        v = v * v
        total = v[:, 0:128]
        for i in range(1, cols // 128):
            total = total + v[:, i * 128 : (i + 1) * 128]
        return total

    def accumulate(origin, block):
        v = rows[origin, block, :]
        ssq[block, :] += folded(v)
        for i in range(4):
            acc[i, block, :] += matmul(v, wgu[i, deep(origin), :])

    def finish(u):
        block = unit(u)
        for origin in (chip(1 - far), chip(far - 1), chip(far)):
            accumulate(origin, block)
        rms = lax.rsqrt(jnp.sum(ssq[block, :], axis=1, keepdims=True) / width + 1e-06)
        for i in range(2):
            g = acc[i, block, :] * rms
            v = acc[2 + i, block, :] * rms
            hid[block, i * ff : (i + 1) * ff] = (g / (1.0 + jnp.exp(-g)) * v).astype(BF16)

    def product(u, chunk):
        return matmul(hid[unit(u), :], wd[:, deep(chunk)])

    def sum_copy(r, d, u):
        block = unit(u) if r > 0 else piece(u, d)
        return remote(
            sbuf.at[d, r, block], rbuf.at[d, r, block], r_s, r_r.at[d, r, u],
            column(1 if d == 0 else n_y - 1),
        )

    def first_sums(u):
        partial = product(u, chip(far)).astype(BF16)
        for d in range(2):
            sbuf[d, 0, piece(u, d), :] = partial[d * (size // 2) : (d + 1) * (size // 2)]
            sum_copy(0, d, u).start()

    def next_sums(r, u):
        for d in range(2):
            partial = product(u, chip(far - r if d == 0 else r - far))
            sum_copy(r - 1, d, u).wait_recv()
            if r == 1:
                here, there = (piece(u, 0), piece(u, 1)) if d == 0 else (piece(u, 1), piece(u, 0))
                parts = (partial[0 : size // 2], partial[size // 2 :])
                sbuf[d, r, here, :] = (parts[d] + rbuf[d, 0, here, :].astype(F32)).astype(BF16)
                sbuf[d, r, there, :] = parts[1 - d].astype(BF16)
            else:
                partial = partial + rbuf[d, r - 1, unit(u), :].astype(F32)
                sbuf[d, r, unit(u), :] = partial.astype(BF16)
            sum_copy(r, d, u).start()

    came = pl.ds(pl.multiple_of(c * slots + sp * per, per), per)

    def send_back(u):
        partial = product(u, y)
        for d in range(2):
            sum_copy(far - 1, d, u).wait_recv()
            partial = partial + rbuf[d, far - 1, unit(u), :].astype(F32)
        for t in range(2):
            eo[t, unit(u), :] = partial[:, t * narrow : (t + 1) * narrow].astype(BF16)
        for place_j in range(2 * u, 2 * u + 2):
            for i in range(n_x):
                spot = place_j * n_x + i
                dst = above(ORDER[place_j]) * n_x + i

                def send(t):
                    remote(eo.at[t, at(spot)], back.at[came], b_s, b_r, (dst, y * 2 + t)).start()

                send_far = functools.partial(send, other)
                send_near = functools.partial(send, c)
                send_far()
                if place_j == 0:
                    pl.when(x != i)(send_near)
                else:
                    send_near()

    everything = pl.ds(0, slots)
    for u in range(UNITS):
        for k in range(2 * u * n_x, 2 * (u + 1) * n_x):
            spot = rows.at[y, at(k)]
            pltpu.make_async_copy(spot, spot, d_r.at[k]).wait()
        for d in range(2):
            hop(1, d, u).start()

    for load in loads[1:4]:
        load.wait()
    for copy in swap_w:
        copy.wait_recv()
    accumulate(y, everything)

    def pass_on(h, u):
        for d in range(2):
            hop_in(h, d, u).wait_recv()
            hop(h + 1, d, u).start()

    def through(u):
        for d in range(2):
            hop_in(far, d, u).wait_recv()
        finish(u)
        first_sums(u)

    for h in range(1, far - 1):
        for u in range(UNITS):
            pass_on(h, u)
        accumulate(chip(-h), everything)
        accumulate(chip(h), everything)
    behind = 3
    for u in range(UNITS + behind):
        if u < UNITS:
            pass_on(far - 1, u)
        if u >= behind:
            through(u - behind)

    for r in range(1, far):
        for u in range(UNITS):
            next_sums(r, u)
    for u in range(UNITS):
        send_back(u)

    stay = pltpu.make_async_copy(eo.at[c, at(x)], back.at[came], l_sem.at[5])
    stay.start()
    stay.wait()
    swap_upd.wait_recv()
    most = pl.ds(0, 2 * slots - per)
    pltpu.make_async_copy(back.at[most], back.at[most], b_r).wait()

    combined = wts[0] * matmul(takes[0], back[...]) + wts[1] * matmul(takes[1], back[...])
    for t in range(2):
        block = slice(t * half, (t + 1) * half)
        out[block, :] = (updx[t] + combined[block]).astype(BF16)

    @pl.when(sp < n_sp - 1)
    def _():
        for copy in halo:
            copy.wait_send()

    for copy in swap_w + [swap_pk, swap_tg, swap_ub, swap_upd]:
        copy.wait_send()
    pltpu.make_async_copy(wc.at[:, own_pair], wc.at[:, own_pair], x_s).wait()
    pltpu.make_async_copy(wc.at[:, own_rows], wc.at[:, own_rows], c_s).wait()
    many = pl.ds(0, n_y - 1)
    pltpu.make_async_copy(wc.at[many, own_pair], wc.at[many, own_pair], w_s).wait()
    pltpu.make_async_copy(stats.at[many], stats.at[many], st_s).wait()
    pltpu.make_async_copy(devs.at[many], devs.at[many], a_s).wait()
    fewer = pl.ds(0, slots - per)
    pltpu.make_async_copy(gath.at[fewer], gath.at[fewer], d_s).wait()
    pltpu.make_async_copy(rows.at[many], rows.at[many], g_s).wait()
    pltpu.make_async_copy(rows.at[many], rows.at[many], r_s).wait()
    pltpu.make_async_copy(back.at[most], back.at[most], b_s).wait()


def solution(mesh):
    n_sp, n_y = mesh.shape["sp"], mesh.shape["tp"] // 2

    def local(cv, cg, taps, gain, ow, res, ids, rw, eg, eu, ed):
        tok, ch = cv.shape
        width = res.shape[1]
        cols = width // n_y
        ff = eg.shape[2]
        slots = tok * ids.shape[1]
        half = tok // 2
        vm, hbm = pl.BlockSpec(memory_space=pltpu.VMEM), pl.BlockSpec(memory_space=pl.ANY)
        dma = pltpu.SemaphoreType.DMA
        scratch = [
            pltpu.VMEM((ch, tok), BF16),
            pltpu.VMEM((ch, tok), BF16),
            pltpu.VMEM(taps.shape, BF16),
            pltpu.VMEM((1, ch), F32),
            pltpu.VMEM(ids.shape[::-1], jnp.int32),
            pltpu.VMEM(rw.shape[::-1], F32),
            pltpu.VMEM((HALO + tok, 2 * ch), BF16),
            pltpu.VMEM((HALO + tok, 2 * ch), BF16),
            pltpu.VMEM((40, 2 * ch), F32),
            pltpu.VMEM((40, 2 * ch), F32),
            pltpu.VMEM((HALO + half, 2 * ch), F32),
            pltpu.VMEM((n_y, 8, half), F32),
            pltpu.VMEM((n_y, 2 * ch, half), F32),
            pltpu.VMEM((n_y, 2 * ch, half), BF16),
            pltpu.VMEM((n_y, 2 * ch, cols), BF16),
            pltpu.VMEM((half, cols), BF16),
            pltpu.VMEM((half, cols), F32),
            pltpu.VMEM((2, half, cols // 2), F32),
            pltpu.VMEM((half, cols // 2), F32),
            pltpu.VMEM((tok, cols), BF16),
            pltpu.VMEM((slots, tok), BF16),
            pltpu.VMEM((2, tok, 2 * slots), BF16),
            pltpu.VMEM((2, tok, 128), F32),
            pltpu.VMEM((slots // UNITS, cols), BF16),
            pltpu.VMEM((slots, cols), BF16),
            pltpu.VMEM((n_y, slots, cols), BF16),
            pltpu.VMEM((4, width, ff), BF16),
            pltpu.VMEM((2 * ff, width), BF16),
            pltpu.VMEM((4, slots, ff), F32),
            pltpu.VMEM((slots, 128), F32),
            pltpu.VMEM((slots, 2 * ff), BF16),
            pltpu.VMEM((2, n_y // 2, slots, cols), BF16),
            pltpu.VMEM((2, n_y // 2, slots, cols), BF16),
            pltpu.VMEM((2, slots, cols // 2), BF16),
            pltpu.VMEM((2 * slots, cols // 2), BF16),
            dma((12,)), dma((8,)), dma((8,)), dma((2,)), dma((2,)),
            dma, dma((n_y,)), dma, dma((n_y,)), dma, dma((n_y + 1,)),
            dma, dma((n_y,)), dma, dma((n_y,)),
            dma, dma((n_sp,)), dma, dma((2, n_y // 2, UNITS)), dma, dma((2, n_y // 2, UNITS)),
            dma, dma,
            pltpu.SemaphoreType.REGULAR((STREAMS // 2,)),
        ]
        return pl.pallas_call(
            functools.partial(layer, n_sp, n_y),
            out_shape=jax.ShapeDtypeStruct((tok, cols // 2), BF16),
            in_specs=[hbm] * 11,
            out_specs=vm,
            scratch_shapes=scratch,
            compiler_params=pltpu.CompilerParams(
                collective_id=0, has_side_effects=True, vmem_limit_bytes=56 << 20
            ),
        )(cv.T, cg.T, taps, gain.reshape(1, ch), ow, res, ids.T, rw.T, eg, eu, ed)

    placed = (
        P("sp", "tp"), P("sp", "tp"), P(None, "tp"), P("tp"), P("tp", None), P("sp", None),
        P("sp", None), P("sp", None), P("sp", None, "tp"), P("sp", None, "tp"), P("sp", "tp", None),
    )
    return jax.shard_map(local, mesh=mesh, in_specs=placed, out_specs=P("sp", "tp"), check_vma=False)
```

```python
import functools

import jax
import jax.numpy as jnp
from jax import lax
from jax.experimental import pallas as pl
from jax.experimental.pallas import tpu as pltpu
from jax.sharding import PartitionSpec as P

MESH = pl.DeviceIdType.MESH
F32, BF16 = jnp.float32, jnp.bfloat16
HALO = 32
STREAMS = 8
UNITS = 4
ORDER = (0, 7, 3, 4, 2, 5, 1, 6)
SENDING = (0, 7, 4, 3, 5, 2, 6, 1)


def iota(shape, dim):
    return lax.broadcasted_iota(jnp.int32, shape, dim)


def matmul(a, b, precision=None):
    return jnp.dot(a, b, preferred_element_type=F32, precision=precision)


def matmul_t(a, b):
    return lax.dot_general(a, b, (((0,), (0,)), ((), ())), preferred_element_type=F32)


def layer(
    n_sp, n_y,
    cv_in, cg_in, taps_in, gain_in, ow, res, ids_in, rw_in, eg, eu, ed,
    out,
    cv, cg, taps, gain, ids, rw, owv, pk_own, pk_par, tg_own, tg_par, gext, stats, gcol, devs, wc, resv, upd, updx, ups, ub, gs, takes, wts,
    first_rows, gath, rows, wgu, wd, acc, ssq, hid, sbuf, rbuf, eo, back,
    l_sem, sw_s, sw_r, h_s, h_r, w_s, w_r, st_s, st_r, a_s, a_r, x_s, x_r, c_s, c_r, d_s, d_r, g_s, g_r,
    r_s, r_r, b_s, b_r, tok_sem,
):
    sp, tp = lax.axis_index("sp"), lax.axis_index("tp")
    y, c = tp // 2, tp % 2
    other = 1 - c
    n_x = n_sp // STREAMS
    z, x = sp // n_x, sp % n_x
    partner = (sp, y * 2 + other)
    ch, tok = cv.shape
    half = tok // 2
    wide = 2 * ch
    width = res.shape[1]
    cols = width // n_y
    ff = eg.shape[2]
    slots = gath.shape[0]
    per = slots // n_sp
    size = slots // UNITS
    far = n_y // 2

    def column(k):
        return (sp, lax.rem(y + k, n_y) * 2 + c)

    def chip(k):
        return lax.rem(y + n_y + k, n_y)

    def remote(src, dst, s, r, dev):
        return pltpu.make_async_remote_copy(
            src_ref=src, dst_ref=dst, send_sem=s, recv_sem=r, device_id=dev, device_id_type=MESH
        )

    barrier = pltpu.get_barrier_semaphore()

    def greet(dev):
        pl.semaphore_signal(barrier, inc=1, device_id=dev, device_id_type=MESH)

    nxt = lax.rem(sp + 1, n_sp)
    prv = lax.rem(sp + n_sp - 1, n_sp)
    z_next = (lax.rem(z + 1, STREAMS) * n_x + x, tp)
    z_prev = (lax.rem(z + STREAMS - 1, STREAMS) * n_x + x, tp)
    near = [column(k) for k in range(n_y - 1, 0, -1)]
    for i in range(1, n_x):
        side = z * n_x + lax.rem(x + i, n_x)
        near += [(side, tp), (side, y * 2 + other)]
    near += [z_next, z_prev, partner]
    for dev in near:
        greet(dev)

    @pl.when(sp < n_sp - 1)
    def _():
        greet((nxt, tp))
        greet((nxt, y * 2 + other))

    @pl.when(sp > 0)
    def _():
        greet((prv, tp))
        greet((prv, y * 2 + other))

    ends = jnp.where(sp > 0, 2, 0) + jnp.where(sp < n_sp - 1, 2, 0)

    def token(r):
        for dev in (z_next, z_prev):
            pl.semaphore_signal(tok_sem.at[r], inc=1, device_id=dev, device_id_type=MESH)

    my_cols = pl.ds(pl.multiple_of(y * cols, cols), cols)
    my_half = pl.ds(pl.multiple_of(c * half, half), half)
    own_rows = pl.ds(pl.multiple_of(c * ch, ch), ch)
    half_ch = ch // 2
    pair_x = sp + 1 - 2 * (x % 2)
    pair_rows = pl.ds(pl.multiple_of((x % 2) * half_ch, half_ch), half_ch)
    own_pair = pl.ds(pl.multiple_of(c * ch + (x % 2) * half_ch, half_ch), half_ch)
    small = [
        pltpu.make_async_copy(src, dst, l_sem.at[6 + i])
        for i, (src, dst) in enumerate(
            ((cv_in, cv), (cg_in, cg), (taps_in, taps), (gain_in, gain), (ids_in, ids), (rw_in, rw))
        )
    ]
    loads = [
        pltpu.make_async_copy(res.at[my_half, my_cols], resv, l_sem.at[0]),
        pltpu.make_async_copy(eg.at[0], wgu.at[0], l_sem.at[1]),
        pltpu.make_async_copy(eu.at[0], wgu.at[2], l_sem.at[2]),
        pltpu.make_async_copy(ed.at[0], wd.at[pl.ds(0, ff)], l_sem.at[3]),
    ]
    bring_ow = pltpu.make_async_copy(ow.at[pair_rows], owv, l_sem.at[12])
    for load in small + [bring_ow] + loads:
        load.start()

    lane = iota((ch, wide), 1)
    chan = iota((ch, wide), 0)
    put_low = (lane == chan).astype(BF16)
    put_high = (lane == chan + ch).astype(BF16)
    for load in small[0:4]:
        load.wait()
    pk_own[pl.ds(HALO, tok), :] = (
        matmul_t(cv[...], put_low) + matmul_t(cg[...], put_high)
    ).astype(BF16)
    n_taps = taps.shape[0]
    tg_own[...] = jnp.zeros_like(tg_own)
    tg_own[pl.ds(0, n_taps), :] = matmul(taps[...], put_low)
    tg_own[pl.ds(n_taps, 1), :] = matmul(
        jnp.broadcast_to(gain[...], (8, ch)), put_low.astype(F32), lax.Precision.HIGHEST
    )[0:1]

    pl.semaphore_wait(barrier, len(near) + ends)

    body = pl.ds(HALO, tok)
    head = pl.ds(0, HALO)
    tail = pl.ds(tok, HALO)
    halo = [
        remote(pk_own.at[tail], pk_own.at[head], h_s.at[0], h_r.at[0], (nxt, tp)),
        remote(pk_own.at[tail], pk_par.at[head], h_s.at[1], h_r.at[1], (nxt, y * 2 + other)),
    ]

    @pl.when(sp < n_sp - 1)
    def _():
        for copy in halo:
            copy.start()

    @pl.when(sp == 0)
    def _():
        pk_own[head, :] = jnp.zeros((HALO, wide), BF16)
        pk_par[head, :] = jnp.zeros((HALO, wide), BF16)

    swap_tg = remote(tg_own, tg_par, sw_s.at[1], sw_r.at[1], partner)
    swap_pk = remote(pk_own.at[body], pk_par.at[body], sw_s.at[0], sw_r.at[0], partner)
    swap_tg.start()
    swap_pk.start()

    outward = (1, n_y - 1, 2, n_y - 2, 3, n_y - 3, far)
    bring_ow.wait()
    keep_w = pltpu.make_async_copy(owv.at[:, my_cols], wc.at[y, own_pair], l_sem.at[4])
    keep_w.start()
    inward = (far, 3, n_y - 3, 2, n_y - 2, 1, n_y - 1)
    for k in inward:
        far_cols = pl.ds(pl.multiple_of(chip(k) * cols, cols), cols)
        remote(owv.at[:, far_cols], wc.at[y, own_pair], w_s, w_r.at[y], column(k)).start()

    token(0)
    swap_w = [
        remote(eg.at[0], wgu.at[1], sw_s.at[2], sw_r.at[2], partner),
        remote(eu.at[0], wgu.at[3], sw_s.at[3], sw_r.at[3], partner),
        remote(ed.at[0], wd.at[pl.ds(ff, ff)], sw_s.at[4], sw_r.at[4], partner),
    ]
    for load in small[4:6]:
        load.wait()
    expert = iota((128, tok), 0)
    id0, id1 = ids[0:1, :], ids[1:2, :]
    hot0, hot1 = (id0 == expert).astype(F32), (id1 == expert).astype(F32)
    before = (iota((tok, tok), 0) < iota((tok, tok), 1)).astype(BF16)
    earlier = matmul((hot0 + hot1).astype(BF16), before)
    place = iota((slots, tok), 0) + c * slots
    slot_rows = []
    for ident, hot in ((id0, hot0), (id1, hot1)):
        rank = jnp.sum(earlier * hot, axis=0, keepdims=True).astype(jnp.int32)
        slot_rows.append(jnp.where(rank < per, 0, slots - per) + ident * per + rank)
    gs[...] = jnp.where((place == slot_rows[0]) | (place == slot_rows[1]), 1.0, 0.0).astype(BF16)

    lane2, chan2 = iota((wide, wide), 1), iota((wide, wide), 0)

    def pick(first, to):
        return (
            (chan2 >= first) & (chan2 < first + ch) & (lane2 == chan2 - first + to * ch)
        ).astype(BF16)

    swap_tg.wait_recv()
    tg = matmul(tg_own[...], pick(0, c).astype(F32), lax.Precision.HIGHEST) + matmul(
        tg_par[...], pick(0, other).astype(F32), lax.Precision.HIGHEST
    )

    def everywhere(buf, s, r):
        @pl.loop(1, n_y)
        def _(k):
            remote(buf.at[y], buf.at[y], s, r.at[y], column(k)).start()

    def arrived(buf, s, r, k):
        origin = lax.rem(y + k, n_y)
        remote(buf.at[origin], buf.at[origin], s, r.at[origin], column(k)).wait_recv()
        return origin

    def tokens(r):
        pl.semaphore_wait(tok_sem.at[r], 2)
        if r < STREAMS // 2 - 1:
            token(r + 1)

    tokens(0)
    swap_pk.wait_recv()

    @pl.when(sp > 0)
    def _():
        for copy in halo:
            copy.wait_recv()

    span = pl.ds(pl.multiple_of(c * half, half), half + HALO)
    mine, theirs = pk_own[span, :], pk_par[span, :]
    value = matmul(mine, pick(0, c)) + matmul(theirs, pick(0, other))
    gate = matmul(mine, pick(ch, c)) + matmul(theirs, pick(ch, other))
    gated = value / (1.0 + jnp.exp(-gate))
    start = (iota(gated.shape, 0) < HALO) & (sp == 0) & (c == 0)
    gext[...] = jnp.where(start, 0.0, gated)
    filtered = jnp.zeros((half, wide), F32)
    for i in range(n_taps):
        filtered = filtered + tg[i : i + 1, :] * gext[pl.ds(i + HALO + 1 - n_taps, half), :]

    turned = jnp.transpose(filtered)
    mean = jnp.sum(turned, axis=0, keepdims=True) / wide
    turned = turned - mean
    spread = jnp.sum(turned * turned, axis=0, keepdims=True) / wide
    devs[y] = turned.astype(BF16)
    line = iota((8, half), 0)
    note = jnp.where(line == 1, spread, jnp.broadcast_to(tg[n_taps : n_taps + 1, :], (8, half)))
    stats[y] = jnp.where(line == 0, mean, note)
    everywhere(stats, st_s, st_r)

    def tell(origin, k, r):
        remote(devs.at[origin], devs.at[origin], a_s, r, column(k)).start()

    for k in (2, n_y - 2, 1, n_y - 1):
        tell(y, k, a_r.at[y])
    tokens(1)

    def hear(k):
        origin = lax.rem(y + k, n_y)
        remote(devs.at[origin], devs.at[origin], a_s, a_r.at[origin], partner).wait_recv()
        return origin

    def share(k):
        block = wc.at[chip(k), own_pair]
        if k == 0:
            keep_w.wait()
        else:
            remote(block, block, w_s, w_r.at[chip(k)], partner).wait_recv()
        remote(block, block, x_s, x_r.at[chip(k)], (pair_x, tp)).start()

    for k in (0, 1, n_y - 1, 2, n_y - 2, 3, n_y - 3, far):
        share(k)
    for k, on in ((n_y - 2, 1), (2, n_y - 1)):
        origin = hear(k)
        tell(origin, on, a_r.at[origin])
        piece_of = devs.at[origin, pl.ds(0 if on == 1 else ch, ch)]
        sem = a_r.at[origin] if on == 1 else a_r.at[n_y]
        remote(piece_of, piece_of, a_s, sem, column(2 if on == 1 else n_y - 2)).start()
    tokens(2)

    @pl.loop(1, n_y)
    def _(k):
        arrived(stats, st_s, st_r, k)

    average = stats[0, 0:1, :]
    for o in range(1, n_y):
        average = average + stats[o, 0:1, :]
    average = average / n_y
    variance = jnp.zeros_like(average)
    for o in range(n_y):
        gap = stats[o, 0:1, :] - average
        variance = variance + (stats[o, 1:2, :] + gap * gap)
    scale = lax.rsqrt(variance / n_y + 1e-05)
    for o in range(n_y):
        gcol[o] = jnp.transpose(jnp.broadcast_to(stats[o, 2:3, :], (half, wide))) * scale

    def mixed(origin):
        shift = stats[origin, 0:1, :] - average
        normed = (devs[origin].astype(F32) + shift) * gcol[origin]
        activated = (normed / (1.0 + jnp.exp(-normed))).astype(BF16)
        return matmul_t(activated, wc[origin])

    for k in (0,) + outward:
        block = wc.at[chip(k), own_pair]
        remote(block, block, x_s, x_r.at[chip(k)], partner).wait_recv()
        block = wc.at[chip(k), own_rows]
        remote(block, block, c_s, c_r.at[chip(k)], partner).start()

    def whole(k):
        block = wc.at[chip(k), own_rows]
        remote(block, block, c_s, c_r.at[chip(k)], partner).wait_recv()
        return chip(k)

    loads[0].wait()
    whole(0)
    upd[...] = resv[...].astype(F32) + mixed(y)
    for k in outward[0:6]:
        if k not in (2, n_y - 2):
            hear(k)
        upd[...] += mixed(whole(k))
    last_half = devs.at[chip(far), pl.ds(0, ch)]
    for sem in (a_r.at[chip(far)], a_r.at[n_y]):
        remote(last_half, last_half, a_s, sem, partner).wait_recv()
    upd[...] += mixed(whole(far))

    ub[my_half, :] = upd[...].astype(BF16)
    swap_ub = remote(ub.at[my_half], ub.at[my_half], sw_s.at[6], sw_r.at[6], partner)
    swap_ub.start()
    narrow = cols // 2
    for t in range(2):

        @pl.when(c == t)
        def _():
            updx[t] = upd[:, t * narrow : (t + 1) * narrow]
            ups[...] = upd[:, (1 - t) * narrow : (2 - t) * narrow]

    swap_upd = remote(ups, updx.at[c], sw_s.at[7], sw_r.at[7], partner)
    swap_upd.start()
    for copy in swap_w:
        copy.start()
    swap_ub.wait_recv()

    tokens(3)

    def at(k):
        return pl.ds(pl.multiple_of(k * per, per), per)

    def below(j):
        return lax.rem(z + STREAMS - j, STREAMS)

    def above(j):
        return lax.rem(z + j, STREAMS)

    block_z = n_x * per
    for turn_j, j in enumerate(SENDING):
        place_j = ORDER.index(j)
        spot = place_j * n_x + x
        to_z = pl.ds(pl.multiple_of(below(j) * block_z, block_z), block_z)
        if place_j < 2:
            picked = matmul(gs[to_z, :], ub[...]).astype(BF16)
            first_rows[pl.ds(place_j * block_z, block_z), :] = picked
        elif turn_j == 2:
            gath[...] = matmul(gs[...], ub[...]).astype(BF16)
        for i in range(n_x):
            dst = below(j) * n_x + lax.rem(x + i, n_x)
            if place_j < 2:
                start_at = place_j * block_z + lax.rem(x + i, n_x) * per
                src = first_rows.at[pl.ds(pl.multiple_of(start_at, per), per)]
            else:
                src = gath.at[at(dst)]
            if i == 0 and j == 0:
                keep = pltpu.make_async_copy(src, rows.at[y, at(spot)], d_r.at[spot])
                keep.start()
            else:
                remote(src, rows.at[y, at(spot)], d_s, d_r.at[spot], (dst, tp)).start()

    for k in range(2):
        wts[k] = jnp.transpose(jnp.broadcast_to(rw[k : k + 1, :], (128, tok)))
        slot = jnp.transpose(jnp.broadcast_to(slot_rows[k].astype(F32), (128, tok)))
        for m in range(2 * slots // 128):
            here = (iota((tok, 128), 1) + m * 128).astype(F32)
            takes[k, :, m * 128 : (m + 1) * 128] = jnp.where(slot == here, 1.0, 0.0).astype(BF16)

    acc[...] = jnp.zeros_like(acc)
    ssq[...] = jnp.zeros_like(ssq)

    def unit(u):
        return pl.ds(u * size, size)

    def piece(u, d):
        return pl.ds(u * size + d * (size // 2), size // 2)

    def hop(h, d, u):
        origin = chip(1 - h if d == 0 else h - 1)
        block = rows.at[origin, unit(u) if h < far else piece(u, d)]
        return remote(block, block, g_s, g_r.at[d, h - 1, u], column(1 if d == 0 else n_y - 1))

    def hop_in(h, d, u):
        origin = chip(-h if d == 0 else h)
        block = rows.at[origin, unit(u) if h < far else piece(u, d)]
        return remote(block, block, g_s, g_r.at[d, h - 1, u], partner)

    def deep(origin):
        return pl.ds(pl.multiple_of(origin * cols, cols), cols)

    def folded(v):
        v = v.astype(F32)
        v = v * v
        total = v[:, 0:128]
        for i in range(1, cols // 128):
            total = total + v[:, i * 128 : (i + 1) * 128]
        return total

    def accumulate(origin, block):
        v = rows[origin, block, :]
        ssq[block, :] += folded(v)
        for i in range(4):
            acc[i, block, :] += matmul(v, wgu[i, deep(origin), :])

    def finish(u):
        block = unit(u)
        accumulate(chip(far), block)
        rms = lax.rsqrt(jnp.sum(ssq[block, :], axis=1, keepdims=True) / width + 1e-06)
        for i in range(2):
            g = acc[i, block, :] * rms
            v = acc[2 + i, block, :] * rms
            hid[block, i * ff : (i + 1) * ff] = (g / (1.0 + jnp.exp(-g)) * v).astype(BF16)

    def product(u, chunk):
        return matmul(hid[unit(u), :], wd[:, deep(chunk)])

    def sum_copy(r, d, u):
        block = unit(u) if r > 0 else piece(u, d)
        return remote(
            sbuf.at[d, r, block], rbuf.at[d, r, block], r_s, r_r.at[d, r, u],
            column(1 if d == 0 else n_y - 1),
        )

    def first_sums(u):
        partial = product(u, chip(far)).astype(BF16)
        for d in range(2):
            sbuf[d, 0, piece(u, d), :] = partial[d * (size // 2) : (d + 1) * (size // 2)]
            sum_copy(0, d, u).start()

    def next_sums(r, u):
        for d in range(2):
            partial = product(u, chip(far - r if d == 0 else r - far))
            sum_copy(r - 1, d, u).wait_recv()
            if r == 1:
                here, there = (piece(u, 0), piece(u, 1)) if d == 0 else (piece(u, 1), piece(u, 0))
                parts = (partial[0 : size // 2], partial[size // 2 :])
                sbuf[d, r, here, :] = (parts[d] + rbuf[d, 0, here, :].astype(F32)).astype(BF16)
                sbuf[d, r, there, :] = parts[1 - d].astype(BF16)
            else:
                partial = partial + rbuf[d, r - 1, unit(u), :].astype(F32)
                sbuf[d, r, unit(u), :] = partial.astype(BF16)
            sum_copy(r, d, u).start()

    came = pl.ds(pl.multiple_of(c * slots + sp * per, per), per)

    def send_back(u):
        partial = product(u, y)
        for d in range(2):
            sum_copy(far - 1, d, u).wait_recv()
            partial = partial + rbuf[d, far - 1, unit(u), :].astype(F32)
        for t in range(2):
            eo[t, unit(u), :] = partial[:, t * narrow : (t + 1) * narrow].astype(BF16)
        for place_j in range(2 * u, 2 * u + 2):
            for i in range(n_x):
                spot = place_j * n_x + i
                dst = above(ORDER[place_j]) * n_x + i

                def send(t):
                    remote(eo.at[t, at(spot)], back.at[came], b_s, b_r, (dst, y * 2 + t)).start()

                send_far = functools.partial(send, other)
                send_near = functools.partial(send, c)
                send_far()
                if place_j == 0:
                    pl.when(x != i)(send_near)
                else:
                    send_near()

    everything = pl.ds(0, slots)
    for u in range(UNITS):
        for k in range(2 * u * n_x, 2 * (u + 1) * n_x):
            spot = rows.at[y, at(k)]
            pltpu.make_async_copy(spot, spot, d_r.at[k]).wait()
        for d in range(2):
            hop(1, d, u).start()

    for load in loads[1:4]:
        load.wait()
    for copy in swap_w:
        copy.wait_recv()
    accumulate(y, everything)

    def pass_on(h, u):
        for d in range(2):
            hop_in(h, d, u).wait_recv()
            hop(h + 1, d, u).start()

    def through(u):
        for d in range(2):
            hop_in(far, d, u).wait_recv()
        finish(u)
        first_sums(u)

    for h in range(1, far - 1):
        for u in range(UNITS):
            pass_on(h, u)
        accumulate(chip(-h), everything)
        accumulate(chip(h), everything)
    behind = 3
    for u in range(UNITS + behind):
        if u < UNITS:
            pass_on(far - 1, u)
            accumulate(chip(1 - far), unit(u))
            accumulate(chip(far - 1), unit(u))
        if u >= behind:
            through(u - behind)

    for r in range(1, far):
        for u in range(UNITS):
            next_sums(r, u)
    for u in range(UNITS):
        send_back(u)

    stay = pltpu.make_async_copy(eo.at[c, at(x)], back.at[came], l_sem.at[5])
    stay.start()
    stay.wait()
    swap_upd.wait_recv()
    most = pl.ds(0, 2 * slots - per)
    pltpu.make_async_copy(back.at[most], back.at[most], b_r).wait()

    combined = wts[0] * matmul(takes[0], back[...]) + wts[1] * matmul(takes[1], back[...])
    for t in range(2):
        block = slice(t * half, (t + 1) * half)
        out[block, :] = (updx[t] + combined[block]).astype(BF16)

    @pl.when(sp < n_sp - 1)
    def _():
        for copy in halo:
            copy.wait_send()

    for copy in swap_w + [swap_pk, swap_tg, swap_ub, swap_upd]:
        copy.wait_send()
    pltpu.make_async_copy(wc.at[:, own_pair], wc.at[:, own_pair], x_s).wait()
    pltpu.make_async_copy(wc.at[:, own_rows], wc.at[:, own_rows], c_s).wait()
    many = pl.ds(0, n_y - 1)
    pltpu.make_async_copy(wc.at[many, own_pair], wc.at[many, own_pair], w_s).wait()
    pltpu.make_async_copy(stats.at[many], stats.at[many], st_s).wait()
    pltpu.make_async_copy(devs.at[many], devs.at[many], a_s).wait()
    fewer = pl.ds(0, slots - per)
    pltpu.make_async_copy(gath.at[fewer], gath.at[fewer], d_s).wait()
    pltpu.make_async_copy(rows.at[many], rows.at[many], g_s).wait()
    pltpu.make_async_copy(rows.at[many], rows.at[many], r_s).wait()
    pltpu.make_async_copy(back.at[most], back.at[most], b_s).wait()


def solution(mesh):
    n_sp, n_y = mesh.shape["sp"], mesh.shape["tp"] // 2

    def local(cv, cg, taps, gain, ow, res, ids, rw, eg, eu, ed):
        tok, ch = cv.shape
        width = res.shape[1]
        cols = width // n_y
        ff = eg.shape[2]
        slots = tok * ids.shape[1]
        half = tok // 2
        vm, hbm = pl.BlockSpec(memory_space=pltpu.VMEM), pl.BlockSpec(memory_space=pl.ANY)
        dma = pltpu.SemaphoreType.DMA
        scratch = [
            pltpu.VMEM((ch, tok), BF16),
            pltpu.VMEM((ch, tok), BF16),
            pltpu.VMEM(taps.shape, BF16),
            pltpu.VMEM((1, ch), F32),
            pltpu.VMEM(ids.shape[::-1], jnp.int32),
            pltpu.VMEM(rw.shape[::-1], F32),
            pltpu.VMEM((ch // 2, width), BF16),
            pltpu.VMEM((HALO + tok, 2 * ch), BF16),
            pltpu.VMEM((HALO + tok, 2 * ch), BF16),
            pltpu.VMEM((40, 2 * ch), F32),
            pltpu.VMEM((40, 2 * ch), F32),
            pltpu.VMEM((HALO + half, 2 * ch), F32),
            pltpu.VMEM((n_y, 8, half), F32),
            pltpu.VMEM((n_y, 2 * ch, half), F32),
            pltpu.VMEM((n_y, 2 * ch, half), BF16),
            pltpu.VMEM((n_y, 2 * ch, cols), BF16),
            pltpu.VMEM((half, cols), BF16),
            pltpu.VMEM((half, cols), F32),
            pltpu.VMEM((2, half, cols // 2), F32),
            pltpu.VMEM((half, cols // 2), F32),
            pltpu.VMEM((tok, cols), BF16),
            pltpu.VMEM((slots, tok), BF16),
            pltpu.VMEM((2, tok, 2 * slots), BF16),
            pltpu.VMEM((2, tok, 128), F32),
            pltpu.VMEM((slots // UNITS, cols), BF16),
            pltpu.VMEM((slots, cols), BF16),
            pltpu.VMEM((n_y, slots, cols), BF16),
            pltpu.VMEM((4, width, ff), BF16),
            pltpu.VMEM((2 * ff, width), BF16),
            pltpu.VMEM((4, slots, ff), F32),
            pltpu.VMEM((slots, 128), F32),
            pltpu.VMEM((slots, 2 * ff), BF16),
            pltpu.VMEM((2, n_y // 2, slots, cols), BF16),
            pltpu.VMEM((2, n_y // 2, slots, cols), BF16),
            pltpu.VMEM((2, slots, cols // 2), BF16),
            pltpu.VMEM((2 * slots, cols // 2), BF16),
            dma((13,)), dma((8,)), dma((8,)), dma((2,)), dma((2,)),
            dma, dma((n_y,)), dma, dma((n_y,)), dma, dma((n_y + 1,)),
            dma, dma((n_y,)), dma, dma((n_y,)),
            dma, dma((n_sp,)), dma, dma((2, n_y // 2, UNITS)), dma, dma((2, n_y // 2, UNITS)),
            dma, dma,
            pltpu.SemaphoreType.REGULAR((STREAMS // 2,)),
        ]
        return pl.pallas_call(
            functools.partial(layer, n_sp, n_y),
            out_shape=jax.ShapeDtypeStruct((tok, cols // 2), BF16),
            in_specs=[hbm] * 11,
            out_specs=vm,
            scratch_shapes=scratch,
            compiler_params=pltpu.CompilerParams(
                collective_id=0, has_side_effects=True, vmem_limit_bytes=56 << 20
            ),
        )(cv.T, cg.T, taps, gain.reshape(1, ch), ow, res, ids.T, rw.T, eg, eu, ed)

    placed = (
        P("sp", "tp"), P("sp", "tp"), P(None, "tp"), P("tp"), P("tp", None), P("sp", None),
        P("sp", None), P("sp", None), P("sp", None, "tp"), P("sp", None, "tp"), P("sp", "tp", None),
    )
    return jax.shard_map(local, mesh=mesh, in_specs=placed, out_specs=P("sp", "tp"), check_vma=False)
```

```python
import functools

import jax
import jax.numpy as jnp
from jax import lax
from jax.experimental import pallas as pl
from jax.experimental.pallas import tpu as pltpu
from jax.sharding import PartitionSpec as P

MESH = pl.DeviceIdType.MESH
F32, BF16 = jnp.float32, jnp.bfloat16
HALO = 32
STREAMS = 8
UNITS = 4
ORDER = (0, 7, 3, 4, 2, 5, 1, 6)
SENDING = (0, 7, 4, 3, 5, 2, 6, 1)


def iota(shape, dim):
    return lax.broadcasted_iota(jnp.int32, shape, dim)


def matmul(a, b, precision=None):
    return jnp.dot(a, b, preferred_element_type=F32, precision=precision)


def matmul_t(a, b):
    return lax.dot_general(a, b, (((0,), (0,)), ((), ())), preferred_element_type=F32)


def layer(
    n_sp, n_y,
    cv_in, cg_in, taps_in, gain_in, ow, res, ids_in, rw_in, eg, eu, ed,
    out,
    cv, cg, taps, gain, ids, rw, owv, pk_own, pk_par, tg_own, tg_par, gext, stats, gcol, devs, wc, resv, upd, updx, ups, ub, gs, takes, wts,
    first_rows, gath, rows, wgu, wd, acc, ssq, hid, sbuf, rbuf, eo, back,
    l_sem, sw_s, sw_r, h_s, h_r, w_s, w_r, st_s, st_r, a_s, a_r, x_s, x_r, c_s, c_r, d_s, d_r, g_s, g_r,
    r_s, r_r, b_s, b_r, tok_sem,
):
    sp, tp = lax.axis_index("sp"), lax.axis_index("tp")
    y, c = tp // 2, tp % 2
    other = 1 - c
    n_x = n_sp // STREAMS
    z, x = sp // n_x, sp % n_x
    partner = (sp, y * 2 + other)
    ch, tok = cv.shape
    half = tok // 2
    wide = 2 * ch
    width = res.shape[1]
    cols = width // n_y
    ff = eg.shape[2]
    slots = gath.shape[0]
    per = slots // n_sp
    size = slots // UNITS
    far = n_y // 2

    def column(k):
        return (sp, lax.rem(y + k, n_y) * 2 + c)

    def chip(k):
        return lax.rem(y + n_y + k, n_y)

    def remote(src, dst, s, r, dev):
        return pltpu.make_async_remote_copy(
            src_ref=src, dst_ref=dst, send_sem=s, recv_sem=r, device_id=dev, device_id_type=MESH
        )

    barrier = pltpu.get_barrier_semaphore()

    def greet(dev):
        pl.semaphore_signal(barrier, inc=1, device_id=dev, device_id_type=MESH)

    nxt = lax.rem(sp + 1, n_sp)
    prv = lax.rem(sp + n_sp - 1, n_sp)
    z_next = (lax.rem(z + 1, STREAMS) * n_x + x, tp)
    z_prev = (lax.rem(z + STREAMS - 1, STREAMS) * n_x + x, tp)
    near = [column(k) for k in range(n_y - 1, 0, -1)]
    for i in range(1, n_x):
        side = z * n_x + lax.rem(x + i, n_x)
        near += [(side, tp), (side, y * 2 + other)]
    near += [z_next, z_prev, partner]
    for dev in near:
        greet(dev)

    @pl.when(sp < n_sp - 1)
    def _():
        greet((nxt, tp))
        greet((nxt, y * 2 + other))

    @pl.when(sp > 0)
    def _():
        greet((prv, tp))
        greet((prv, y * 2 + other))

    ends = jnp.where(sp > 0, 2, 0) + jnp.where(sp < n_sp - 1, 2, 0)

    def token(r):
        for dev in (z_next, z_prev):
            pl.semaphore_signal(tok_sem.at[r], inc=1, device_id=dev, device_id_type=MESH)

    my_cols = pl.ds(pl.multiple_of(y * cols, cols), cols)
    my_half = pl.ds(pl.multiple_of(c * half, half), half)
    own_rows = pl.ds(pl.multiple_of(c * ch, ch), ch)
    half_ch = ch // 2
    pair_x = sp + 1 - 2 * (x % 2)
    pair_rows = pl.ds(pl.multiple_of((x % 2) * half_ch, half_ch), half_ch)
    own_pair = pl.ds(pl.multiple_of(c * ch + (x % 2) * half_ch, half_ch), half_ch)
    small = [
        pltpu.make_async_copy(src, dst, l_sem.at[6 + i])
        for i, (src, dst) in enumerate(
            ((cv_in, cv), (cg_in, cg), (taps_in, taps), (gain_in, gain), (ids_in, ids), (rw_in, rw))
        )
    ]
    loads = [
        pltpu.make_async_copy(res.at[my_half, my_cols], resv, l_sem.at[0]),
        pltpu.make_async_copy(eg.at[0], wgu.at[0], l_sem.at[1]),
        pltpu.make_async_copy(eu.at[0], wgu.at[2], l_sem.at[2]),
        pltpu.make_async_copy(ed.at[0], wd.at[pl.ds(0, ff)], l_sem.at[3]),
    ]
    bring_ow = pltpu.make_async_copy(ow.at[pair_rows], owv, l_sem.at[12])
    for load in small + [bring_ow] + loads:
        load.start()

    lane = iota((ch, wide), 1)
    chan = iota((ch, wide), 0)
    put_low = (lane == chan).astype(BF16)
    put_high = (lane == chan + ch).astype(BF16)
    for load in small[0:4]:
        load.wait()
    pk_own[pl.ds(HALO, tok), :] = (
        matmul_t(cv[...], put_low) + matmul_t(cg[...], put_high)
    ).astype(BF16)
    n_taps = taps.shape[0]
    tg_own[...] = jnp.zeros_like(tg_own)
    tg_own[pl.ds(0, n_taps), :] = matmul(taps[...], put_low)
    tg_own[pl.ds(n_taps, 1), :] = matmul(
        jnp.broadcast_to(gain[...], (8, ch)), put_low.astype(F32), lax.Precision.HIGHEST
    )[0:1]

    pl.semaphore_wait(barrier, len(near) + ends)

    body = pl.ds(HALO, tok)
    head = pl.ds(0, HALO)
    tail = pl.ds(tok, HALO)
    halo = [
        remote(pk_own.at[tail], pk_own.at[head], h_s.at[0], h_r.at[0], (nxt, tp)),
        remote(pk_own.at[tail], pk_par.at[head], h_s.at[1], h_r.at[1], (nxt, y * 2 + other)),
    ]

    @pl.when(sp < n_sp - 1)
    def _():
        for copy in halo:
            copy.start()

    @pl.when(sp == 0)
    def _():
        pk_own[head, :] = jnp.zeros((HALO, wide), BF16)
        pk_par[head, :] = jnp.zeros((HALO, wide), BF16)

    swap_tg = remote(tg_own, tg_par, sw_s.at[1], sw_r.at[1], partner)
    swap_pk = remote(pk_own.at[body], pk_par.at[body], sw_s.at[0], sw_r.at[0], partner)
    swap_tg.start()
    swap_pk.start()

    outward = (1, n_y - 1, 2, n_y - 2, 3, n_y - 3, far)
    bring_ow.wait()
    keep_w = pltpu.make_async_copy(owv.at[:, my_cols], wc.at[y, own_pair], l_sem.at[4])
    keep_w.start()
    inward = (far, 3, n_y - 3, 2, n_y - 2, 1, n_y - 1)
    for k in inward:
        far_cols = pl.ds(pl.multiple_of(chip(k) * cols, cols), cols)
        remote(owv.at[:, far_cols], wc.at[y, own_pair], w_s, w_r.at[y], column(k)).start()

    token(0)
    swap_w = [
        remote(eg.at[0], wgu.at[1], sw_s.at[2], sw_r.at[2], partner),
        remote(eu.at[0], wgu.at[3], sw_s.at[3], sw_r.at[3], partner),
        remote(ed.at[0], wd.at[pl.ds(ff, ff)], sw_s.at[4], sw_r.at[4], partner),
    ]
    for load in small[4:6]:
        load.wait()
    expert = iota((128, tok), 0)
    id0, id1 = ids[0:1, :], ids[1:2, :]
    hot0, hot1 = (id0 == expert).astype(F32), (id1 == expert).astype(F32)
    before = (iota((tok, tok), 0) < iota((tok, tok), 1)).astype(BF16)
    earlier = matmul((hot0 + hot1).astype(BF16), before)
    place = iota((slots, tok), 0) + c * slots
    slot_rows = []
    for ident, hot in ((id0, hot0), (id1, hot1)):
        rank = jnp.sum(earlier * hot, axis=0, keepdims=True).astype(jnp.int32)
        slot_rows.append(jnp.where(rank < per, 0, slots - per) + ident * per + rank)
    gs[...] = jnp.where((place == slot_rows[0]) | (place == slot_rows[1]), 1.0, 0.0).astype(BF16)

    lane2, chan2 = iota((wide, wide), 1), iota((wide, wide), 0)

    def pick(first, to):
        return (
            (chan2 >= first) & (chan2 < first + ch) & (lane2 == chan2 - first + to * ch)
        ).astype(BF16)

    swap_tg.wait_recv()
    tg = matmul(tg_own[...], pick(0, c).astype(F32), lax.Precision.HIGHEST) + matmul(
        tg_par[...], pick(0, other).astype(F32), lax.Precision.HIGHEST
    )

    def everywhere(buf, s, r):
        @pl.loop(1, n_y)
        def _(k):
            remote(buf.at[y], buf.at[y], s, r.at[y], column(k)).start()

    def arrived(buf, s, r, k):
        origin = lax.rem(y + k, n_y)
        remote(buf.at[origin], buf.at[origin], s, r.at[origin], column(k)).wait_recv()
        return origin

    def tokens(r):
        pl.semaphore_wait(tok_sem.at[r], 2)
        if r < STREAMS // 2 - 1:
            token(r + 1)

    tokens(0)
    swap_pk.wait_recv()

    @pl.when(sp > 0)
    def _():
        for copy in halo:
            copy.wait_recv()

    span = pl.ds(pl.multiple_of(c * half, half), half + HALO)
    mine, theirs = pk_own[span, :], pk_par[span, :]
    value = matmul(mine, pick(0, c)) + matmul(theirs, pick(0, other))
    gate = matmul(mine, pick(ch, c)) + matmul(theirs, pick(ch, other))
    gated = value / (1.0 + jnp.exp(-gate))
    start = (iota(gated.shape, 0) < HALO) & (sp == 0) & (c == 0)
    gext[...] = jnp.where(start, 0.0, gated)
    filtered = jnp.zeros((half, wide), F32)
    for i in range(n_taps):
        filtered = filtered + tg[i : i + 1, :] * gext[pl.ds(i + HALO + 1 - n_taps, half), :]

    turned = jnp.transpose(filtered)
    mean = jnp.sum(turned, axis=0, keepdims=True) / wide
    turned = turned - mean
    spread = jnp.sum(turned * turned, axis=0, keepdims=True) / wide
    devs[y] = turned.astype(BF16)
    line = iota((8, half), 0)
    note = jnp.where(line == 1, spread, jnp.broadcast_to(tg[n_taps : n_taps + 1, :], (8, half)))
    stats[y] = jnp.where(line == 0, mean, note)
    everywhere(stats, st_s, st_r)

    def tell(origin, k, r):
        remote(devs.at[origin], devs.at[origin], a_s, r, column(k)).start()

    for k in (2, n_y - 2, 1, n_y - 1):
        tell(y, k, a_r.at[y])
    tokens(1)

    def hear(k):
        origin = lax.rem(y + k, n_y)
        remote(devs.at[origin], devs.at[origin], a_s, a_r.at[origin], partner).wait_recv()
        return origin

    def share(k):
        block = wc.at[chip(k), own_pair]
        if k == 0:
            keep_w.wait()
        else:
            remote(block, block, w_s, w_r.at[chip(k)], partner).wait_recv()
        remote(block, block, x_s, x_r.at[chip(k)], (pair_x, tp)).start()

    for k in (0, 1, n_y - 1, 2, n_y - 2, 3, n_y - 3, far):
        share(k)
    for k, on in ((n_y - 2, 1), (2, n_y - 1)):
        origin = hear(k)
        tell(origin, on, a_r.at[origin])
        piece_of = devs.at[origin, pl.ds(0 if on == 1 else ch, ch)]
        sem = a_r.at[origin] if on == 1 else a_r.at[n_y]
        remote(piece_of, piece_of, a_s, sem, column(2 if on == 1 else n_y - 2)).start()
    tokens(2)

    @pl.loop(1, n_y)
    def _(k):
        arrived(stats, st_s, st_r, k)

    average = stats[0, 0:1, :]
    for o in range(1, n_y):
        average = average + stats[o, 0:1, :]
    average = average / n_y
    variance = jnp.zeros_like(average)
    for o in range(n_y):
        gap = stats[o, 0:1, :] - average
        variance = variance + (stats[o, 1:2, :] + gap * gap)
    scale = lax.rsqrt(variance / n_y + 1e-05)
    for o in range(n_y):
        gcol[o] = jnp.transpose(jnp.broadcast_to(stats[o, 2:3, :], (half, wide))) * scale

    def mixed(origin):
        shift = stats[origin, 0:1, :] - average
        normed = (devs[origin].astype(F32) + shift) * gcol[origin]
        activated = (normed / (1.0 + jnp.exp(-normed))).astype(BF16)
        return matmul_t(activated, wc[origin])

    for k in (0,) + outward:
        block = wc.at[chip(k), own_pair]
        remote(block, block, x_s, x_r.at[chip(k)], partner).wait_recv()
        block = wc.at[chip(k), own_rows]
        remote(block, block, c_s, c_r.at[chip(k)], partner).start()

    def whole(k):
        block = wc.at[chip(k), own_rows]
        remote(block, block, c_s, c_r.at[chip(k)], partner).wait_recv()
        return chip(k)

    loads[0].wait()
    whole(0)
    upd[...] = resv[...].astype(F32) + mixed(y)
    for k in outward[0:6]:
        if k not in (2, n_y - 2):
            hear(k)
        upd[...] += mixed(whole(k))
    last_half = devs.at[chip(far), pl.ds(0, ch)]
    for sem in (a_r.at[chip(far)], a_r.at[n_y]):
        remote(last_half, last_half, a_s, sem, partner).wait_recv()
    upd[...] += mixed(whole(far))

    ub[my_half, :] = upd[...].astype(BF16)
    swap_ub = remote(ub.at[my_half], ub.at[my_half], sw_s.at[6], sw_r.at[6], partner)
    swap_ub.start()
    narrow = cols // 2
    for t in range(2):

        @pl.when(c == t)
        def _():
            updx[t] = upd[:, t * narrow : (t + 1) * narrow]
            ups[...] = upd[:, (1 - t) * narrow : (2 - t) * narrow]

    swap_upd = remote(ups, updx.at[c], sw_s.at[7], sw_r.at[7], partner)
    swap_upd.start()
    swap_ub.wait_recv()

    tokens(3)

    def at(k):
        return pl.ds(pl.multiple_of(k * per, per), per)

    def below(j):
        return lax.rem(z + STREAMS - j, STREAMS)

    def above(j):
        return lax.rem(z + j, STREAMS)

    block_z = n_x * per
    for turn_j, j in enumerate(SENDING):
        place_j = ORDER.index(j)
        spot = place_j * n_x + x
        to_z = pl.ds(pl.multiple_of(below(j) * block_z, block_z), block_z)
        if place_j < 2:
            picked = matmul(gs[to_z, :], ub[...]).astype(BF16)
            first_rows[pl.ds(place_j * block_z, block_z), :] = picked
        elif turn_j == 2:
            gath[...] = matmul(gs[...], ub[...]).astype(BF16)
        for i in range(n_x):
            dst = below(j) * n_x + lax.rem(x + i, n_x)
            if place_j < 2:
                start_at = place_j * block_z + lax.rem(x + i, n_x) * per
                src = first_rows.at[pl.ds(pl.multiple_of(start_at, per), per)]
            else:
                src = gath.at[at(dst)]
            if i == 0 and j == 0:
                keep = pltpu.make_async_copy(src, rows.at[y, at(spot)], d_r.at[spot])
                keep.start()
            else:
                remote(src, rows.at[y, at(spot)], d_s, d_r.at[spot], (dst, tp)).start()

    for copy in swap_w:
        copy.start()

    for k in range(2):
        wts[k] = jnp.transpose(jnp.broadcast_to(rw[k : k + 1, :], (128, tok)))
        slot = jnp.transpose(jnp.broadcast_to(slot_rows[k].astype(F32), (128, tok)))
        for m in range(2 * slots // 128):
            here = (iota((tok, 128), 1) + m * 128).astype(F32)
            takes[k, :, m * 128 : (m + 1) * 128] = jnp.where(slot == here, 1.0, 0.0).astype(BF16)

    acc[...] = jnp.zeros_like(acc)
    ssq[...] = jnp.zeros_like(ssq)

    def unit(u):
        return pl.ds(u * size, size)

    def piece(u, d):
        return pl.ds(u * size + d * (size // 2), size // 2)

    def hop(h, d, u):
        origin = chip(1 - h if d == 0 else h - 1)
        block = rows.at[origin, unit(u) if h < far else piece(u, d)]
        return remote(block, block, g_s, g_r.at[d, h - 1, u], column(1 if d == 0 else n_y - 1))

    def hop_in(h, d, u):
        origin = chip(-h if d == 0 else h)
        block = rows.at[origin, unit(u) if h < far else piece(u, d)]
        return remote(block, block, g_s, g_r.at[d, h - 1, u], partner)

    def deep(origin):
        return pl.ds(pl.multiple_of(origin * cols, cols), cols)

    def folded(v):
        v = v.astype(F32)
        v = v * v
        total = v[:, 0:128]
        for i in range(1, cols // 128):
            total = total + v[:, i * 128 : (i + 1) * 128]
        return total

    def accumulate(origin, block):
        v = rows[origin, block, :]
        ssq[block, :] += folded(v)
        for i in range(4):
            acc[i, block, :] += matmul(v, wgu[i, deep(origin), :])

    def finish(u):
        block = unit(u)
        accumulate(chip(far), block)
        rms = lax.rsqrt(jnp.sum(ssq[block, :], axis=1, keepdims=True) / width + 1e-06)
        for i in range(2):
            g = acc[i, block, :] * rms
            v = acc[2 + i, block, :] * rms
            hid[block, i * ff : (i + 1) * ff] = (g / (1.0 + jnp.exp(-g)) * v).astype(BF16)

    def product(u, chunk):
        return matmul(hid[unit(u), :], wd[:, deep(chunk)])

    def sum_copy(r, d, u):
        block = unit(u) if r > 0 else piece(u, d)
        return remote(
            sbuf.at[d, r, block], rbuf.at[d, r, block], r_s, r_r.at[d, r, u],
            column(1 if d == 0 else n_y - 1),
        )

    def first_sums(u):
        partial = product(u, chip(far)).astype(BF16)
        for d in range(2):
            sbuf[d, 0, piece(u, d), :] = partial[d * (size // 2) : (d + 1) * (size // 2)]
            sum_copy(0, d, u).start()

    def next_sums(r, u):
        for d in range(2):
            partial = product(u, chip(far - r if d == 0 else r - far))
            sum_copy(r - 1, d, u).wait_recv()
            if r == 1:
                here, there = (piece(u, 0), piece(u, 1)) if d == 0 else (piece(u, 1), piece(u, 0))
                parts = (partial[0 : size // 2], partial[size // 2 :])
                sbuf[d, r, here, :] = (parts[d] + rbuf[d, 0, here, :].astype(F32)).astype(BF16)
                sbuf[d, r, there, :] = parts[1 - d].astype(BF16)
            else:
                partial = partial + rbuf[d, r - 1, unit(u), :].astype(F32)
                sbuf[d, r, unit(u), :] = partial.astype(BF16)
            sum_copy(r, d, u).start()

    came = pl.ds(pl.multiple_of(c * slots + sp * per, per), per)

    def send_back(u):
        partial = product(u, y)
        for d in range(2):
            sum_copy(far - 1, d, u).wait_recv()
            partial = partial + rbuf[d, far - 1, unit(u), :].astype(F32)
        for t in range(2):
            eo[t, unit(u), :] = partial[:, t * narrow : (t + 1) * narrow].astype(BF16)
        for place_j in range(2 * u, 2 * u + 2):
            for i in range(n_x):
                spot = place_j * n_x + i
                dst = above(ORDER[place_j]) * n_x + i

                def send(t):
                    remote(eo.at[t, at(spot)], back.at[came], b_s, b_r, (dst, y * 2 + t)).start()

                send_far = functools.partial(send, other)
                send_near = functools.partial(send, c)
                send_far()
                if place_j == 0:
                    pl.when(x != i)(send_near)
                else:
                    send_near()

    everything = pl.ds(0, slots)
    def pass_on(h, u):
        for d in range(2):
            hop_in(h, d, u).wait_recv()
            hop(h + 1, d, u).start()

    def enter(u):
        for k in range(2 * u * n_x, 2 * (u + 1) * n_x):
            spot = rows.at[y, at(k)]
            pltpu.make_async_copy(spot, spot, d_r.at[k]).wait()
        for d in range(2):
            hop(1, d, u).start()

    def through(u):
        for d in range(2):
            hop_in(far, d, u).wait_recv()
        finish(u)
        first_sums(u)

    for u in range(UNITS - 1):
        enter(u)
    pass_on(1, 0)
    enter(UNITS - 1)

    for load in loads[1:4]:
        load.wait()
    for copy in swap_w:
        copy.wait_recv()
    accumulate(y, everything)


    for h in range(1, far - 1):
        for u in range(1 if h == 1 else 0, UNITS):
            pass_on(h, u)
        accumulate(chip(-h), everything)
        accumulate(chip(h), everything)
    behind = 3
    for u in range(UNITS + behind):
        if u < UNITS:
            pass_on(far - 1, u)
            accumulate(chip(1 - far), unit(u))
            accumulate(chip(far - 1), unit(u))
        if u >= behind:
            through(u - behind)

    for r in range(1, far):
        for u in range(UNITS):
            next_sums(r, u)
    for u in range(UNITS):
        send_back(u)

    stay = pltpu.make_async_copy(eo.at[c, at(x)], back.at[came], l_sem.at[5])
    stay.start()
    stay.wait()
    swap_upd.wait_recv()
    most = pl.ds(0, 2 * slots - per)
    pltpu.make_async_copy(back.at[most], back.at[most], b_r).wait()

    combined = wts[0] * matmul(takes[0], back[...]) + wts[1] * matmul(takes[1], back[...])
    for t in range(2):
        block = slice(t * half, (t + 1) * half)
        out[block, :] = (updx[t] + combined[block]).astype(BF16)

    @pl.when(sp < n_sp - 1)
    def _():
        for copy in halo:
            copy.wait_send()

    for copy in swap_w + [swap_pk, swap_tg, swap_ub, swap_upd]:
        copy.wait_send()
    pltpu.make_async_copy(wc.at[:, own_pair], wc.at[:, own_pair], x_s).wait()
    pltpu.make_async_copy(wc.at[:, own_rows], wc.at[:, own_rows], c_s).wait()
    many = pl.ds(0, n_y - 1)
    pltpu.make_async_copy(wc.at[many, own_pair], wc.at[many, own_pair], w_s).wait()
    pltpu.make_async_copy(stats.at[many], stats.at[many], st_s).wait()
    pltpu.make_async_copy(devs.at[many], devs.at[many], a_s).wait()
    fewer = pl.ds(0, slots - per)
    pltpu.make_async_copy(gath.at[fewer], gath.at[fewer], d_s).wait()
    pltpu.make_async_copy(rows.at[many], rows.at[many], g_s).wait()
    pltpu.make_async_copy(rows.at[many], rows.at[many], r_s).wait()
    pltpu.make_async_copy(back.at[most], back.at[most], b_s).wait()


def solution(mesh):
    n_sp, n_y = mesh.shape["sp"], mesh.shape["tp"] // 2

    def local(cv, cg, taps, gain, ow, res, ids, rw, eg, eu, ed):
        tok, ch = cv.shape
        width = res.shape[1]
        cols = width // n_y
        ff = eg.shape[2]
        slots = tok * ids.shape[1]
        half = tok // 2
        vm, hbm = pl.BlockSpec(memory_space=pltpu.VMEM), pl.BlockSpec(memory_space=pl.ANY)
        dma = pltpu.SemaphoreType.DMA
        scratch = [
            pltpu.VMEM((ch, tok), BF16),
            pltpu.VMEM((ch, tok), BF16),
            pltpu.VMEM(taps.shape, BF16),
            pltpu.VMEM((1, ch), F32),
            pltpu.VMEM(ids.shape[::-1], jnp.int32),
            pltpu.VMEM(rw.shape[::-1], F32),
            pltpu.VMEM((ch // 2, width), BF16),
            pltpu.VMEM((HALO + tok, 2 * ch), BF16),
            pltpu.VMEM((HALO + tok, 2 * ch), BF16),
            pltpu.VMEM((40, 2 * ch), F32),
            pltpu.VMEM((40, 2 * ch), F32),
            pltpu.VMEM((HALO + half, 2 * ch), F32),
            pltpu.VMEM((n_y, 8, half), F32),
            pltpu.VMEM((n_y, 2 * ch, half), F32),
            pltpu.VMEM((n_y, 2 * ch, half), BF16),
            pltpu.VMEM((n_y, 2 * ch, cols), BF16),
            pltpu.VMEM((half, cols), BF16),
            pltpu.VMEM((half, cols), F32),
            pltpu.VMEM((2, half, cols // 2), F32),
            pltpu.VMEM((half, cols // 2), F32),
            pltpu.VMEM((tok, cols), BF16),
            pltpu.VMEM((slots, tok), BF16),
            pltpu.VMEM((2, tok, 2 * slots), BF16),
            pltpu.VMEM((2, tok, 128), F32),
            pltpu.VMEM((slots // UNITS, cols), BF16),
            pltpu.VMEM((slots, cols), BF16),
            pltpu.VMEM((n_y, slots, cols), BF16),
            pltpu.VMEM((4, width, ff), BF16),
            pltpu.VMEM((2 * ff, width), BF16),
            pltpu.VMEM((4, slots, ff), F32),
            pltpu.VMEM((slots, 128), F32),
            pltpu.VMEM((slots, 2 * ff), BF16),
            pltpu.VMEM((2, n_y // 2, slots, cols), BF16),
            pltpu.VMEM((2, n_y // 2, slots, cols), BF16),
            pltpu.VMEM((2, slots, cols // 2), BF16),
            pltpu.VMEM((2 * slots, cols // 2), BF16),
            dma((13,)), dma((8,)), dma((8,)), dma((2,)), dma((2,)),
            dma, dma((n_y,)), dma, dma((n_y,)), dma, dma((n_y + 1,)),
            dma, dma((n_y,)), dma, dma((n_y,)),
            dma, dma((n_sp,)), dma, dma((2, n_y // 2, UNITS)), dma, dma((2, n_y // 2, UNITS)),
            dma, dma,
            pltpu.SemaphoreType.REGULAR((STREAMS // 2,)),
        ]
        return pl.pallas_call(
            functools.partial(layer, n_sp, n_y),
            out_shape=jax.ShapeDtypeStruct((tok, cols // 2), BF16),
            in_specs=[hbm] * 11,
            out_specs=vm,
            scratch_shapes=scratch,
            compiler_params=pltpu.CompilerParams(
                collective_id=0, has_side_effects=True, vmem_limit_bytes=56 << 20
            ),
        )(cv.T, cg.T, taps, gain.reshape(1, ch), ow, res, ids.T, rw.T, eg, eu, ed)

    placed = (
        P("sp", "tp"), P("sp", "tp"), P(None, "tp"), P("tp"), P("tp", None), P("sp", None),
        P("sp", None), P("sp", None), P("sp", None, "tp"), P("sp", None, "tp"), P("sp", "tp", None),
    )
    return jax.shard_map(local, mesh=mesh, in_specs=placed, out_specs=P("sp", "tp"), check_vma=False)
```
